512 devices in a mesh: gr: 2 (over z_hi), sp: 32 (over z_lo, y), tp: 8 (over x, core).
Axes of the slice: x: 4, y: 4, z: 16 (z_hi: 2, z_lo: 8; z = z_hi * 8 + z_lo), core: 2. Of those that a mesh axis runs over, the one named last changes fastest.
Arguments:
- tokens: bfloat16 [8, 4096, 4096], P('gr', 'sp'), parts along dimension 0, may hold values from -6 to 6
- key_weight: bfloat16 [4096, 2048], P('sp', 'tp'), may hold values from -0.09375 to 0.09375
- value_weight: bfloat16 [4096, 2048], P('sp', 'tp'), may hold values from -0.09375 to 0.09375
- log_decay: float32 [32, 8, 4096], P('tp', 'gr', 'sp'), parts along dimension 1, may hold values from -1 to 0, as said below
- new_query: bfloat16 [8, 2048], P('gr', 'tp'), parts along dimension 0, may hold values from -6 to 6
- new_key: bfloat16 [8, 2048], P('gr', 'tp'), parts along dimension 0, may hold values from -24 to 24
- new_value: bfloat16 [8, 2048], P('gr', 'tp'), parts along dimension 0, may hold values from -6 to 6
- step_decay: float32 [32, 8], P('tp', 'gr'), parts along dimension 1, may hold values from -1.5 to -0.05
- norm_gain: float32 [2048], P('tp'), may hold values from 0.1 to 1.9
Outputs:
- state_cache: float32 [512, 32, 64], P('gr', 'tp'), parts along dimension 0
- first_read: bfloat16 [8, 2048], P('gr', 'tp'), parts along dimension 0
The draws below stay inside these ranges and needn't reach their ends.
There are 2 independent parts, one for each index of `gr`. The reference program is written for one: setup_inputs(seed, part) draws one part's arguments, and reference() takes and returns one part's arrays. A program takes and returns all parts, laid end to end along the dimension named above; an argument that names none is the same for every part. Nothing has to cross between parts.
Inputs may be any that keep to these rules, and one draw needn't show every extreme that they name: `log_decay`: every entry is at most zero.
All inputs are finite; a program needn't handle non-finite values.
Results may differ from the reference program's by a relative error of at most 0.0053.
Values may be sent and summed in bfloat16 or wider, within the bound.
No kernel may reach another device: no remote copies, remote signals or barrier semaphores. Data moves between devices by JAX's collectives and lax.ppermute only.
A program may use at most 64 MiB of HBM per device.

```python
import jax
import jax.numpy as jnp
from jax import lax

D = 4096
RETENTION_HEADS = 32
HEAD_DIM = 64
GROUP_PROMPTS = 4
SPAN = 128
PROMPT_LENGTH = 4096


def draw_log_decay(key, part):
    key_vectors = jax.random.split(jax.random.fold_in(key, 7), 7)
    fast_share = 0.5
    is_fast = jax.random.uniform(key_vectors[0], (RETENTION_HEADS,), jnp.float32) < fast_share
    fast_rate = jnp.exp(jax.random.uniform(key_vectors[1], (RETENTION_HEADS,), jnp.float32, jnp.log(1.0 / 60.0), jnp.log(1.0 / 30.0)))
    slow_rate = jax.random.uniform(key_vectors[2], (RETENTION_HEADS,), jnp.float32, 0.1, 0.5) * jnp.log(10.0) / PROMPT_LENGTH
    decay_speed = jnp.where(is_fast, fast_rate, slow_rate)
    blocks = PROMPT_LENGTH // SPAN
    block_multiplier = jnp.exp(jax.random.uniform(key_vectors[3], (GROUP_PROMPTS, blocks), jnp.float32, jnp.log(0.5), jnp.log(2.0)))
    block_multiplier = jnp.broadcast_to(block_multiplier[:, :, None], (GROUP_PROMPTS, blocks, SPAN)).reshape(GROUP_PROMPTS, PROMPT_LENGTH)
    approximate = jax.random.uniform(key_vectors[4], (RETENTION_HEADS, GROUP_PROMPTS, PROMPT_LENGTH), jnp.float32, 0.5, 1.5)
    surge_position = jax.random.uniform(key_vectors[5], (RETENTION_HEADS, GROUP_PROMPTS, PROMPT_LENGTH), jnp.float32) < 2.0 / PROMPT_LENGTH
    surge_length = jnp.log(jax.random.uniform(key_vectors[6], (RETENTION_HEADS, GROUP_PROMPTS, PROMPT_LENGTH), jnp.float32, 0.5, 0.8))
    decay_factor = -decay_speed[:, None, None] * block_multiplier[None, :, :] * approximate + jnp.where(surge_position, surge_length, 0.0)
    return decay_factor.astype(jnp.float32)


def shard_levels(rng, dims, shards, smallest, top_value):
    def one(dim, parts):
        draws = jax.random.uniform(jax.random.fold_in(jax.random.fold_in(rng, 6), dim), (parts,), jnp.float32, smallest / len(shards), top_value / len(shards))
        return jnp.repeat(jnp.exp(draws), dims[dim] // parts).reshape((-1,) + (1,) * (len(dims) - dim - 1))

    level = one(*shards[0])
    for cut in shards[1:]:
        level = level * one(*cut)
    return level


def normal_values(own_key, dims, deviation, limit, shards=(), held_as=jnp.bfloat16):
    drawn = deviation * jax.random.normal(own_key, dims, jnp.float32)
    if shards:
        drawn = drawn * shard_levels(own_key, dims, shards, -0.22, 0.18)
    return jnp.clip(drawn, -limit, limit).astype(held_as)


def setup_inputs(seed: int = 0, part: int = 0) -> dict:
    key_list = jax.random.split(jax.random.key(seed), 10)
    part_splits = jax.random.split(jax.random.fold_in(key_list[9], part), 10)
    return {
        "tokens": normal_values(part_splits[0], (GROUP_PROMPTS, PROMPT_LENGTH, D), 1.0, 6.0, ((1, 32),)),
        "key_weight": normal_values(key_list[1], (D, RETENTION_HEADS * HEAD_DIM), D ** -0.5, 0.09375, ((0, 32), (1, 8))),
        "value_weight": normal_values(key_list[2], (D, RETENTION_HEADS * HEAD_DIM), D ** -0.5, 0.09375, ((0, 32), (1, 8))),
        "log_decay": draw_log_decay(jax.random.fold_in(jax.random.fold_in(key_list[9], part), 71), part),
        "new_query": normal_values(part_splits[4], (GROUP_PROMPTS, RETENTION_HEADS * HEAD_DIM), 1.0, 6.0, ((1, 8),)),
        "new_key": normal_values(part_splits[5], (GROUP_PROMPTS, RETENTION_HEADS * HEAD_DIM), 4.0, 24.0, ((1, 8),)),
        "new_value": normal_values(part_splits[6], (GROUP_PROMPTS, RETENTION_HEADS * HEAD_DIM), 1.0, 6.0, ((1, 8),)),
        "step_decay": jnp.clip(-1.5 + 1.45 * jax.random.uniform(part_splits[7], (RETENTION_HEADS, GROUP_PROMPTS), jnp.float32) ** shard_levels(part_splits[7], (RETENTION_HEADS, GROUP_PROMPTS), ((0, 8),), -0.2, 0.2), -1.5, -0.05),
        "norm_gain": jnp.clip(1.0 + 0.18 * jax.random.normal(key_list[8], (RETENTION_HEADS * HEAD_DIM,), jnp.float32), 0.1, 1.9),
    }


def rotate_half(values, positions):
    half = values.shape[-1] // 2
    inverse = 10000.0 ** (-jnp.arange(half, dtype=jnp.float32) * (2.0 / values.shape[-1]))
    angles = positions[..., None] * inverse
    cosine = jnp.cos(angles)
    sine = jnp.sin(angles)
    first, second = (values[..., :half], values[..., half:])
    return jnp.concatenate([first * cosine - second * sine, second * cosine + first * sine], axis=-1)

def reference(tokens, key_weight, value_weight, log_decay, new_query, new_key, new_value, step_decay, norm_gain):
    seqs, length, width = tokens.shape
    heads = key_weight.shape[1] // HEAD_DIM
    token_rows = tokens.reshape(seqs * length, width)
    key_vectors = jnp.dot(token_rows, key_weight, preferred_element_type=jnp.float32).astype(jnp.bfloat16)
    values = jnp.dot(token_rows, value_weight, preferred_element_type=jnp.float32).astype(jnp.bfloat16)
    key_vectors = lax.optimization_barrier(key_vectors).astype(jnp.float32).reshape(seqs, length, heads, HEAD_DIM)
    values = lax.optimization_barrier(values).astype(jnp.float32).reshape(seqs, length, heads, HEAD_DIM)
    positions = jnp.arange(length, dtype=jnp.float32)
    rkeys = rotate_half(key_vectors, positions[None, :, None]) * HEAD_DIM ** (-0.5)
    totals = lax.optimization_barrier(jnp.sum(log_decay, axis=-1, keepdims=True))
    weight = jnp.exp(totals - jnp.cumsum(log_decay, axis=-1))
    weight_seq = jnp.transpose(weight, (1, 2, 0))

    def one_prompt(items):
        key_seq, value_seq, decay_seq = items
        weighted = key_seq * decay_seq[:, :, None]
        return jnp.einsum('tha,thb->hab', weighted, value_seq, precision=lax.Precision.HIGHEST)
    prompt_state = lax.map(one_prompt, (rkeys, values, weight_seq))
    end_pos = jnp.full((seqs, heads), float(length), jnp.float32)
    query = rotate_half(new_query.astype(jnp.float32).reshape(seqs, heads, HEAD_DIM), end_pos)
    key_new = rotate_half(new_key.astype(jnp.float32).reshape(seqs, heads, HEAD_DIM), end_pos) * HEAD_DIM ** (-0.5)
    value_new = new_value.astype(jnp.float32).reshape(seqs, heads, HEAD_DIM)
    state = jnp.exp(step_decay).T[:, :, None, None] * prompt_state + key_new[:, :, :, None] * value_new[:, :, None, :]
    raw = jnp.einsum('sha,shab->shb', query, state, precision=lax.Precision.HIGHEST)
    center = lax.optimization_barrier(jnp.mean(raw, axis=-1, keepdims=True))
    spread = lax.optimization_barrier(jnp.mean(jnp.square(raw - center), axis=-1, keepdims=True))
    normed = (raw - center) * lax.rsqrt(spread + 1e-06) * norm_gain.reshape(heads, HEAD_DIM)
    first_read = normed.reshape(seqs, heads * HEAD_DIM).astype(jnp.bfloat16)
    state_cache = jnp.transpose(state, (0, 2, 1, 3)).reshape(seqs * HEAD_DIM, heads, HEAD_DIM)
    return (state_cache, first_read)
```

```python
import jax
import jax.numpy as jnp
from jax import lax
from jax.sharding import PartitionSpec as P

HEAD_DIM = 64


def in_one_piece(arrays, axis, dim, along):
    ends, at = ([], 0)
    for a in arrays[:-1]:
        at += a.shape[along]
        ends.append(at)
    both = jnp.concatenate(arrays, axis=along)
    return tuple(jnp.split(lax.all_gather(both, axis, axis=dim, tiled=True), ends, axis=along))


def copy_for_each(x, axis):
    devices = lax.axis_size(axis)
    return lax.all_to_all(jnp.broadcast_to(x[None], (devices, *x.shape)), axis, 0, 0, tiled=True)


def joined_by_halves(pieces, combine):
    while len(jax.tree.leaves(pieces)[0]) > 1:
        pieces = jax.vmap(combine)(*(pieces[side::2] for side in (0, 1)))
    return pieces[0]


def carried_in(x, axis, combine, identity):
    devices, mine = (lax.axis_size(axis), lax.axis_index(axis))
    passed = jnp.arange(devices) > mine

    def kept(part, zero, own):
        part = jnp.where(
            passed.reshape(-1, *(1 for _ in own.shape)), part, jnp.asarray(zero, own.dtype)
        )
        return part[::-1]

    pieces = copy_for_each(x, axis)
    return joined_by_halves(kept(pieces, identity, x), combine)


def cut_along(x, dim, devices):
    shape = x.shape
    blocks = x.reshape(*shape[:dim], devices, shape[dim] // devices, *shape[dim + 1 :])
    return jnp.moveaxis(blocks, dim, 0)


def sum_at_owner(x, axis, dim):
    blocks = cut_along(x, dim, lax.axis_size(axis))
    arrived = lax.all_to_all(blocks, axis, split_axis=0, concat_axis=0, tiled=True)
    return arrived.sum(axis=0)


def joined_along(blocks, dim):
    shape = list(blocks.shape[1:])
    shape[dim] *= blocks.shape[0]
    return jnp.moveaxis(blocks, 0, dim).reshape(shape)


def gather_directly(x, axis, dim):
    return joined_along(copy_for_each(x, axis), dim)


def rotate_half(values, positions):
    half = values.shape[-1] // 2
    inverse = 10000.0 ** (-jnp.arange(half, dtype=jnp.float32) * (2.0 / values.shape[-1]))
    angles = positions[..., None] * inverse
    cosine = jnp.cos(angles)
    sine = jnp.sin(angles)
    first, second = (values[..., :half], values[..., half:])
    return jnp.concatenate(
        [first * cosine - second * sine, second * cosine + first * sine], axis=-1
    )


def add_totals(earlier, later):
    return earlier + later


def shards(
    tokens,
    key_weight,
    value_weight,
    log_decay,
    new_query,
    new_key,
    new_value,
    step_decay,
    norm_gain,
):
    seqs, span, width = tokens.shape
    heads_here = key_weight.shape[1] // HEAD_DIM
    token_rows = tokens.reshape(seqs * span, width)
    depth = key_weight.shape[0]
    half = depth // lax.axis_size("gr")
    both = jnp.concatenate([key_weight, value_weight], axis=1)
    mine = lax.dynamic_slice_in_dim(both, lax.axis_index("gr") * half, half, 0)
    got = lax.all_gather(mine, ("gr", "sp"), axis=0, tiled=False)
    got = jnp.moveaxis(got.reshape(2, 32, half, both.shape[1]), 0, 1).reshape(32 * depth, -1)
    whole_keys, whole_values = jnp.split(got, 2, axis=1)
    key_sum = jnp.dot(token_rows, whole_keys, preferred_element_type=jnp.float32)
    value_sum = jnp.dot(token_rows, whole_values, preferred_element_type=jnp.float32)
    key_vectors = (
        lax.optimization_barrier(key_sum.astype(jnp.bfloat16))
        .astype(jnp.float32)
        .reshape(seqs, span, heads_here, HEAD_DIM)
    )
    values = (
        lax.optimization_barrier(value_sum.astype(jnp.bfloat16))
        .astype(jnp.float32)
        .reshape(seqs, span, heads_here, HEAD_DIM)
    )
    devices = lax.axis_size("sp")
    offset = lax.axis_index("sp") * span
    positions = (offset + jnp.arange(span, dtype=jnp.int32)).astype(jnp.float32)
    rkeys = rotate_half(key_vectors, positions[None, :, None]) * HEAD_DIM ** (-0.5)
    totals = jnp.sum(log_decay, axis=-1)
    later_sum = carried_in(totals, "sp", add_totals, jnp.zeros_like(totals))
    weight = jnp.exp(totals[:, :, None] - jnp.cumsum(log_decay, axis=-1) + later_sum[:, :, None])
    weighted = rkeys * jnp.transpose(weight, (1, 2, 0))[:, :, :, None]
    term = jnp.einsum("stha,sthb->sahb", weighted, values, precision=lax.Precision.HIGHEST)
    term = term.reshape(seqs * HEAD_DIM, heads_here, HEAD_DIM)
    end_pos = jnp.full((seqs, heads_here), float(span * devices), jnp.float32)
    query = rotate_half(new_query.astype(jnp.float32).reshape(seqs, heads_here, HEAD_DIM), end_pos)
    key_new = rotate_half(
        new_key.astype(jnp.float32).reshape(seqs, heads_here, HEAD_DIM), end_pos
    ) * HEAD_DIM ** (-0.5)
    value_new = new_value.astype(jnp.float32).reshape(seqs, heads_here, HEAD_DIM)
    decay_all = jnp.repeat(jnp.exp(step_decay).T, HEAD_DIM, axis=0)
    key_all = jnp.transpose(key_new, (0, 2, 1)).reshape(seqs * HEAD_DIM, heads_here)
    value_all = jnp.repeat(value_new, HEAD_DIM, axis=0)
    rows = seqs * HEAD_DIM // devices
    owned = sum_at_owner(term, "sp", 0)
    first_row = lax.axis_index("sp") * rows
    decay_rows = lax.dynamic_slice_in_dim(decay_all, first_row, rows, 0)
    key_rows = lax.dynamic_slice_in_dim(key_all, first_row, rows, 0)
    value_rows = lax.dynamic_slice_in_dim(value_all, first_row, rows, 0)
    finished = decay_rows[:, :, None] * owned + key_rows[:, :, None] * value_rows
    state_cache = gather_directly(finished, "sp", 0)
    state_seq = state_cache.reshape(seqs, HEAD_DIM, heads_here, HEAD_DIM)
    raw = jnp.einsum("sha,sahb->shb", query, state_seq, precision=lax.Precision.HIGHEST)
    center = jnp.mean(raw, axis=-1, keepdims=True)
    spread = jnp.mean(jnp.square(raw - center), axis=-1, keepdims=True)
    normed = (raw - center) * lax.rsqrt(spread + 1e-06) * norm_gain.reshape(heads_here, HEAD_DIM)
    first_read = normed.reshape(seqs, heads_here * HEAD_DIM).astype(jnp.bfloat16)
    return (state_cache, first_read)


def solution(mesh):
    placed = (
        P("gr", "sp", None),
        P("sp", "tp"),
        P("sp", "tp"),
        P("tp", "gr", "sp"),
        P("gr", "tp"),
        P("gr", "tp"),
        P("gr", "tp"),
        P("tp", "gr"),
        P("tp"),
    )
    return jax.shard_map(
        shards,
        mesh=mesh,
        in_specs=placed,
        out_specs=(P("gr", "tp", None), P("gr", "tp")),
        check_vma=False,
    )
```

```python
import jax
import jax.numpy as jnp
from jax import lax
from jax.sharding import PartitionSpec as P

HEAD_DIM = 64
Y = 4
PARTS = 3


def rotate_half(values, positions):
    half = values.shape[-1] // 2
    inverse = 10000.0 ** (-jnp.arange(half, dtype=jnp.float32) * (2.0 / values.shape[-1]))
    angles = positions[..., None] * inverse
    cosine = jnp.cos(angles)
    sine = jnp.sin(angles)
    first, second = (values[..., :half], values[..., half:])
    return jnp.concatenate(
        [first * cosine - second * sine, second * cosine + first * sine], axis=-1
    )


def moved_along_z(x, by):
    ring = lax.axis_size("gr") * lax.axis_size("sp") // Y
    pairs = [(z * Y + y, (z + by) % ring * Y + y) for z in range(ring) for y in range(Y)]
    return lax.ppermute(x, ("gr", "sp"), pairs)


def copies_along_y(x):
    groups = [[z * Y + y for y in range(Y)] for z in range(lax.axis_size("sp") // Y)]
    spread = jnp.broadcast_to(x[None], (Y, *x.shape))
    got = lax.all_to_all(spread, "sp", 0, 0, tiled=True, axis_index_groups=groups)
    return got.reshape(Y * x.shape[0], *x.shape[1:])


def projected(token_rows, both):
    planes = lax.axis_size("sp") // Y
    mine = lax.axis_index("sp") // Y
    block = copies_along_y(both)
    depth = block.shape[0]

    def part(weights, plane, start=0):
        first = lax.rem(plane + planes, planes) * depth + start
        cols = lax.dynamic_slice_in_dim(token_rows, first, weights.shape[0], 1)
        return jnp.dot(cols, weights, preferred_element_type=jnp.float32)

    total = part(block, mine)
    up = down = block
    far = planes // 2
    for hop in range(1, far):
        up, down = moved_along_z(up, 1), moved_along_z(down, -1)
        total += part(up, mine - hop) + part(down, mine + hop)
    up, down = moved_along_z(up[: depth // 2], 1), moved_along_z(down[depth // 2 :], -1)
    opposite = jnp.concatenate([up, down], axis=0)
    return total + part(opposite, mine + far)


def in_three(x):
    parts, rest = ([], x)
    for _ in range(PARTS):
        piece = lax.reduce_precision(rest, 8, 7)
        parts.append(piece.astype(jnp.bfloat16))
        rest = rest - piece
    return parts


def shards(
    tokens,
    key_weight,
    value_weight,
    log_decay,
    new_query,
    new_key,
    new_value,
    step_decay,
    norm_gain,
):
    seqs, span, width = tokens.shape
    heads = key_weight.shape[1] // HEAD_DIM
    cols = heads * HEAD_DIM
    lanes = seqs * HEAD_DIM
    devices, mine = (lax.axis_size("sp"), lax.axis_index("sp"))
    rows = cols // devices
    both = jnp.concatenate([key_weight, value_weight], axis=1)
    sums = projected(tokens.reshape(seqs * span, width), both)
    rounded = lax.optimization_barrier(sums.astype(jnp.bfloat16)).astype(jnp.float32)
    keys = rounded[:, :cols].reshape(seqs, span, heads, HEAD_DIM)
    values = rounded[:, cols:].reshape(seqs, span, heads, HEAD_DIM)
    positions = (mine * span + jnp.arange(span, dtype=jnp.int32)).astype(jnp.float32)
    rkeys = rotate_half(keys, positions[None, :, None]) * HEAD_DIM ** (-0.5)
    totals = jnp.sum(log_decay, axis=-1)
    weight = jnp.exp(totals[:, :, None] - jnp.cumsum(log_decay, axis=-1))
    weighted = rkeys * jnp.transpose(weight, (1, 2, 0))[:, :, :, None]
    term = jnp.einsum("sthb,stha->hbsa", values, weighted, precision=lax.Precision.HIGHEST)
    term = term.reshape(devices, rows, lanes).astype(jnp.bfloat16)
    carried = jnp.repeat(jnp.stack(in_three(totals), axis=-1), devices // heads, axis=0)
    carried = carried.reshape(devices, 1, seqs * PARTS)
    carried = jnp.pad(carried, ((0, 0), (0, rows - 1), (0, 128 - seqs * PARTS)))
    sent = jnp.concatenate([term, carried], axis=-1)
    got = lax.all_to_all(sent, "sp", 0, 0, tiled=True)
    their = got[:, 0, lanes : lanes + seqs * PARTS].astype(jnp.float32)
    their = their.reshape(devices, seqs, PARTS).sum(axis=-1)
    after = jnp.arange(devices)[None, :] > jnp.arange(devices)[:, None]
    later = jnp.sum(jnp.where(after[:, :, None], their[None], 0.0), axis=1)
    fade = jnp.repeat(jnp.exp(later), HEAD_DIM, axis=1)
    owned = jnp.sum(got[:, :, :lanes].astype(jnp.float32) * fade[:, None, :], axis=0)

    end_pos = jnp.full((seqs, heads), float(span * devices), jnp.float32)
    query = rotate_half(new_query.astype(jnp.float32).reshape(seqs, heads, HEAD_DIM), end_pos)
    key_new = rotate_half(
        new_key.astype(jnp.float32).reshape(seqs, heads, HEAD_DIM), end_pos
    ) * HEAD_DIM ** (-0.5)
    key_lanes = jnp.transpose(key_new, (1, 0, 2)).reshape(heads, lanes)
    decay_lanes = jnp.repeat(jnp.exp(step_decay), HEAD_DIM, axis=1)
    value_cols = jnp.repeat(new_value.astype(jnp.float32).T, HEAD_DIM, axis=1)
    head = mine // (devices // heads)
    key_row = lax.dynamic_slice_in_dim(key_lanes, head, 1, 0)
    decay_row = lax.dynamic_slice_in_dim(decay_lanes, head, 1, 0)
    value_rows = lax.dynamic_slice_in_dim(value_cols, mine * rows, rows, 0)
    finished = decay_row * owned + key_row * value_rows
    spread = jnp.broadcast_to(finished[None], (devices, rows, lanes))
    state = lax.all_to_all(spread, "sp", 0, 0, tiled=True).reshape(heads, HEAD_DIM, seqs, HEAD_DIM)
    state_cache = jnp.transpose(state.reshape(heads, HEAD_DIM, lanes), (2, 0, 1))
    raw = jnp.einsum("sha,hbsa->shb", query, state, precision=lax.Precision.HIGHEST)
    center = jnp.mean(raw, axis=-1, keepdims=True)
    spread = jnp.mean(jnp.square(raw - center), axis=-1, keepdims=True)
    normed = (raw - center) * lax.rsqrt(spread + 1e-06) * norm_gain.reshape(heads, HEAD_DIM)
    first_read = normed.reshape(seqs, cols).astype(jnp.bfloat16)
    return (state_cache, first_read)


def solution(mesh):
    placed = (
        P("gr", "sp", None),
        P("sp", "tp"),
        P("sp", "tp"),
        P("tp", "gr", "sp"),
        P("gr", "tp"),
        P("gr", "tp"),
        P("gr", "tp"),
        P("tp", "gr"),
        P("tp"),
    )
    return jax.shard_map(
        shards,
        mesh=mesh,
        in_specs=placed,
        out_specs=(P("gr", "tp", None), P("gr", "tp")),
        check_vma=False,
    )
```

```python
import jax
import jax.numpy as jnp
from jax import lax
from jax.sharding import PartitionSpec as P

HEAD_DIM = 64
Y = 4
PARTS = 3


def rotate_half(values, positions):
    half = values.shape[-1] // 2
    inverse = 10000.0 ** (-jnp.arange(half, dtype=jnp.float32) * (2.0 / values.shape[-1]))
    angles = positions[..., None] * inverse
    cosine = jnp.cos(angles)
    sine = jnp.sin(angles)
    first, second = (values[..., :half], values[..., half:])
    return jnp.concatenate(
        [first * cosine - second * sine, second * cosine + first * sine], axis=-1
    )


def moved_along_z(x, by):
    ring = lax.axis_size("gr") * lax.axis_size("sp") // Y
    pairs = [(z * Y + y, (z + by) % ring * Y + y) for z in range(ring) for y in range(Y)]
    return lax.ppermute(x, ("gr", "sp"), pairs)


def copies_along_y(x):
    groups = [[z * Y + y for y in range(Y)] for z in range(lax.axis_size("sp") // Y)]
    spread = jnp.broadcast_to(x[None], (Y, *x.shape))
    got = lax.all_to_all(spread, "sp", 0, 0, tiled=True, axis_index_groups=groups)
    return got.reshape(Y * x.shape[0], *x.shape[1:])


def projected(token_rows, key_weight, value_weight):
    planes = lax.axis_size("sp") // Y
    far = planes // 2
    mine = lax.axis_index("sp").astype(jnp.uint32) // Y
    keys, values = (copies_along_y(key_weight), copies_along_y(value_weight))
    depth = keys.shape[0]

    def part(weights, off):
        first = (mine + (off + planes)) % planes * depth
        cols = lax.dynamic_slice_in_dim(token_rows, first, depth, 1)
        return jnp.dot(cols, weights, preferred_element_type=jnp.float32)

    key_sum, value_sum = (part(keys, 0), part(values, 0))
    key_up, key_down, value_up, value_down = (keys, keys, values, values)
    for hop in range(1, far):
        key_up = moved_along_z(key_up, 1)
        value_down = moved_along_z(value_down, -1)
        value_up = moved_along_z(value_up, 1)
        key_down = moved_along_z(key_down, -1)
        key_sum += part(key_up, -hop) + part(key_down, hop)
        value_sum += part(value_up, -hop) + part(value_down, hop)
    key_sum += part(moved_along_z(key_up, 1), -far)
    value_sum += part(moved_along_z(value_down, -1), far)
    return key_sum, value_sum


def in_three(x):
    parts, rest = ([], x)
    for _ in range(PARTS):
        piece = lax.reduce_precision(rest, 8, 7)
        parts.append(piece.astype(jnp.bfloat16))
        rest = rest - piece
    return parts


def shards(
    tokens,
    key_weight,
    value_weight,
    log_decay,
    new_query,
    new_key,
    new_value,
    step_decay,
    norm_gain,
):
    seqs, span, width = tokens.shape
    heads = key_weight.shape[1] // HEAD_DIM
    cols = heads * HEAD_DIM
    lanes = seqs * HEAD_DIM
    devices, mine = (lax.axis_size("sp"), lax.axis_index("sp"))
    rows = cols // devices
    sums = projected(tokens.reshape(seqs * span, width), key_weight, value_weight)
    keys, values = (
        lax.optimization_barrier(part.astype(jnp.bfloat16))
        .astype(jnp.float32)
        .reshape(seqs, span, heads, HEAD_DIM)
        for part in sums
    )
    positions = (mine * span + jnp.arange(span, dtype=jnp.int32)).astype(jnp.float32)
    rkeys = rotate_half(keys, positions[None, :, None]) * HEAD_DIM ** (-0.5)
    totals = jnp.sum(log_decay, axis=-1)
    weight = jnp.exp(totals[:, :, None] - jnp.cumsum(log_decay, axis=-1))
    weighted = rkeys * jnp.transpose(weight, (1, 2, 0))[:, :, :, None]
    term = jnp.einsum("sthb,stha->hbsa", values, weighted, precision=lax.Precision.HIGHEST)
    term = term.reshape(devices, rows, lanes).astype(jnp.bfloat16)
    carried = jnp.repeat(jnp.stack(in_three(totals), axis=-1), devices // heads, axis=0)
    carried = carried.reshape(devices, 1, seqs * PARTS)
    carried = jnp.pad(carried, ((0, 0), (0, rows - 1), (0, 128 - seqs * PARTS)))
    sent = jnp.concatenate([term, carried], axis=-1)
    got = lax.all_to_all(sent, "sp", 0, 0, tiled=True)
    their = got[:, 0, lanes : lanes + seqs * PARTS].astype(jnp.float32)
    their = their.reshape(devices, seqs, PARTS).sum(axis=-1)
    after = jnp.arange(devices)[None, :] > jnp.arange(devices)[:, None]
    later = jnp.sum(jnp.where(after[:, :, None], their[None], 0.0), axis=1)
    fade = jnp.repeat(jnp.exp(later), HEAD_DIM, axis=1)
    owned = jnp.sum(got[:, :, :lanes].astype(jnp.float32) * fade[:, None, :], axis=0)

    end_pos = jnp.full((seqs, heads), float(span * devices), jnp.float32)
    query = rotate_half(new_query.astype(jnp.float32).reshape(seqs, heads, HEAD_DIM), end_pos)
    key_new = rotate_half(
        new_key.astype(jnp.float32).reshape(seqs, heads, HEAD_DIM), end_pos
    ) * HEAD_DIM ** (-0.5)
    key_lanes = jnp.transpose(key_new, (1, 0, 2)).reshape(heads, lanes)
    decay_lanes = jnp.repeat(jnp.exp(step_decay), HEAD_DIM, axis=1)
    value_cols = jnp.repeat(new_value.astype(jnp.float32).T, HEAD_DIM, axis=1)
    head = mine // (devices // heads)
    key_row = lax.dynamic_slice_in_dim(key_lanes, head, 1, 0)
    decay_row = lax.dynamic_slice_in_dim(decay_lanes, head, 1, 0)
    value_rows = lax.dynamic_slice_in_dim(value_cols, mine * rows, rows, 0)
    finished = decay_row * owned + key_row * value_rows
    spread = jnp.broadcast_to(finished[None], (devices, rows, lanes))
    state = lax.all_to_all(spread, "sp", 0, 0, tiled=True).reshape(heads, HEAD_DIM, seqs, HEAD_DIM)
    state_cache = jnp.transpose(state.reshape(heads, HEAD_DIM, lanes), (2, 0, 1))
    raw = jnp.einsum("sha,hbsa->shb", query, state, precision=lax.Precision.HIGHEST)
    center = jnp.mean(raw, axis=-1, keepdims=True)
    spread = jnp.mean(jnp.square(raw - center), axis=-1, keepdims=True)
    normed = (raw - center) * lax.rsqrt(spread + 1e-06) * norm_gain.reshape(heads, HEAD_DIM)
    first_read = normed.reshape(seqs, cols).astype(jnp.bfloat16)
    return (state_cache, first_read)


def solution(mesh):
    placed = (
        P("gr", "sp", None),
        P("sp", "tp"),
        P("sp", "tp"),
        P("tp", "gr", "sp"),
        P("gr", "tp"),
        P("gr", "tp"),
        P("gr", "tp"),
        P("tp", "gr"),
        P("tp"),
    )
    return jax.shard_map(
        shards,
        mesh=mesh,
        in_specs=placed,
        out_specs=(P("gr", "tp", None), P("gr", "tp")),
        check_vma=False,
    )
```

```python
import jax
import jax.numpy as jnp
from jax import lax
from jax.sharding import PartitionSpec as P

HEAD_DIM = 64
Y = 4
PARTS = 3


def rotate_half(values, positions):
    half = values.shape[-1] // 2
    inverse = 10000.0 ** (-jnp.arange(half, dtype=jnp.float32) * (2.0 / values.shape[-1]))
    angles = positions[..., None] * inverse
    cosine = jnp.cos(angles)
    sine = jnp.sin(angles)
    first, second = (values[..., :half], values[..., half:])
    return jnp.concatenate(
        [first * cosine - second * sine, second * cosine + first * sine], axis=-1
    )


def moved_along_z(x, by):
    ring = lax.axis_size("gr") * lax.axis_size("sp") // Y
    pairs = [(z * Y + y, (z + by) % ring * Y + y) for z in range(ring) for y in range(Y)]
    return lax.ppermute(x, ("gr", "sp"), pairs)


def copies_along_y(arrays):
    groups = [[z * Y + y for y in range(Y)] for z in range(lax.axis_size("sp") // Y)]
    spread = [jnp.broadcast_to(x[None], (Y, *x.shape)) for x in arrays]
    spread = jnp.concatenate(spread, axis=-1)
    got = lax.all_to_all(spread, "sp", 0, 0, tiled=True, axis_index_groups=groups)
    return got.reshape(Y * got.shape[1], got.shape[2])


def projected(token_rows, arrays):
    planes = lax.axis_size("sp") // Y
    far = planes // 2
    mine = lax.axis_index("sp").astype(jnp.uint32) // Y
    block = copies_along_y(arrays)
    depth = block.shape[0]

    def part(weights, off):
        first = (mine + (off + planes)) % planes * depth
        cols = lax.dynamic_slice_in_dim(token_rows, first, depth, 1)
        return jnp.dot(cols, weights, preferred_element_type=jnp.float32)

    total = part(block, 0)
    up = down = block
    for hop in range(1, far):
        up, down = moved_along_z(up, 1), moved_along_z(down, -1)
        total += part(up, -hop) + part(down, hop)
    up, down = moved_along_z(up[: depth // 2], 1), moved_along_z(down[depth // 2 :], -1)
    return total + part(jnp.concatenate([up, down], axis=0), far)


def in_three(x):
    parts, rest = ([], x)
    for _ in range(PARTS):
        piece = lax.reduce_precision(rest, 8, 7)
        parts.append(piece.astype(jnp.bfloat16))
        rest = rest - piece
    return parts


def shards(
    tokens,
    key_weight,
    value_weight,
    log_decay,
    new_query,
    new_key,
    new_value,
    step_decay,
    norm_gain,
):
    seqs, span, width = tokens.shape
    heads = key_weight.shape[1] // HEAD_DIM
    cols = heads * HEAD_DIM
    lanes = seqs * HEAD_DIM
    devices, mine = (lax.axis_size("sp"), lax.axis_index("sp"))
    rows = cols // devices
    sums = projected(tokens.reshape(seqs * span, width), (key_weight, value_weight))
    rounded = lax.optimization_barrier(sums.astype(jnp.bfloat16)).astype(jnp.float32)
    keys = rounded[:, :cols].reshape(seqs, span, heads, HEAD_DIM)
    values = rounded[:, cols:].reshape(seqs, span, heads, HEAD_DIM)
    positions = (mine * span + jnp.arange(span, dtype=jnp.int32)).astype(jnp.float32)
    rkeys = rotate_half(keys, positions[None, :, None]) * HEAD_DIM ** (-0.5)
    totals = jnp.sum(log_decay, axis=-1)
    weight = jnp.exp(totals[:, :, None] - jnp.cumsum(log_decay, axis=-1))
    weighted = rkeys * jnp.transpose(weight, (1, 2, 0))[:, :, :, None]
    term = jnp.einsum("sthb,stha->hbsa", values, weighted, precision=lax.Precision.HIGHEST)
    term = term.reshape(devices, rows, lanes).astype(jnp.bfloat16)
    carried = jnp.repeat(jnp.stack(in_three(totals), axis=-1), devices // heads, axis=0)
    carried = carried.reshape(devices, 1, seqs * PARTS)
    carried = jnp.pad(carried, ((0, 0), (0, rows - 1), (0, 128 - seqs * PARTS)))
    sent = jnp.concatenate([term, carried], axis=-1)
    got = lax.all_to_all(sent, "sp", 0, 0, tiled=True)
    their = got[:, 0, lanes : lanes + seqs * PARTS].astype(jnp.float32)
    their = their.reshape(devices, seqs, PARTS).sum(axis=-1)
    after = jnp.arange(devices)[None, :] > jnp.arange(devices)[:, None]
    later = jnp.sum(jnp.where(after[:, :, None], their[None], 0.0), axis=1)
    fade = jnp.repeat(jnp.exp(later), HEAD_DIM, axis=1)
    owned = jnp.sum(got[:, :, :lanes].astype(jnp.float32) * fade[:, None, :], axis=0)

    end_pos = jnp.full((seqs, heads), float(span * devices), jnp.float32)
    query = rotate_half(new_query.astype(jnp.float32).reshape(seqs, heads, HEAD_DIM), end_pos)
    key_new = rotate_half(
        new_key.astype(jnp.float32).reshape(seqs, heads, HEAD_DIM), end_pos
    ) * HEAD_DIM ** (-0.5)
    key_lanes = jnp.transpose(key_new, (1, 0, 2)).reshape(heads, lanes)
    decay_lanes = jnp.repeat(jnp.exp(step_decay), HEAD_DIM, axis=1)
    value_cols = jnp.repeat(new_value.astype(jnp.float32).T, HEAD_DIM, axis=1)
    head = mine // (devices // heads)
    key_row = lax.dynamic_slice_in_dim(key_lanes, head, 1, 0)
    decay_row = lax.dynamic_slice_in_dim(decay_lanes, head, 1, 0)
    value_rows = lax.dynamic_slice_in_dim(value_cols, mine * rows, rows, 0)
    finished = decay_row * owned + key_row * value_rows
    spread = jnp.broadcast_to(finished.astype(jnp.bfloat16)[None], (devices, rows, lanes))
    state = lax.all_to_all(spread, "sp", 0, 0, tiled=True).astype(jnp.float32)
    state = state.reshape(heads, HEAD_DIM, seqs, HEAD_DIM)
    state_cache = jnp.transpose(state.reshape(heads, HEAD_DIM, lanes), (2, 0, 1))
    raw = jnp.einsum("sha,hbsa->shb", query, state, precision=lax.Precision.HIGHEST)
    center = jnp.mean(raw, axis=-1, keepdims=True)
    spread = jnp.mean(jnp.square(raw - center), axis=-1, keepdims=True)
    normed = (raw - center) * lax.rsqrt(spread + 1e-06) * norm_gain.reshape(heads, HEAD_DIM)
    first_read = normed.reshape(seqs, cols).astype(jnp.bfloat16)
    return (state_cache, first_read)


def solution(mesh):
    placed = (
        P("gr", "sp", None),
        P("sp", "tp"),
        P("sp", "tp"),
        P("tp", "gr", "sp"),
        P("gr", "tp"),
        P("gr", "tp"),
        P("gr", "tp"),
        P("tp", "gr"),
        P("tp"),
    )
    return jax.shard_map(
        shards,
        mesh=mesh,
        in_specs=placed,
        out_specs=(P("gr", "tp", None), P("gr", "tp")),
        check_vma=False,
    )
```

```python
import functools

import jax
import jax.numpy as jnp
from jax import lax
from jax.experimental import pallas as pl
from jax.experimental.pallas import tpu as pltpu
from jax.sharding import PartitionSpec as P

HEAD_DIM = 64
Y = 4
PARTS = 3
EXTRA = 128
EXACT = lax.Precision.HIGHEST
F32, BF16 = (jnp.float32, jnp.bfloat16)


def rotate_half(values, positions):
    half = values.shape[-1] // 2
    inverse = 10000.0 ** (-jnp.arange(half, dtype=jnp.float32) * (2.0 / values.shape[-1]))
    angles = positions[..., None] * inverse
    cosine = jnp.cos(angles)
    sine = jnp.sin(angles)
    first, second = (values[..., :half], values[..., half:])
    return jnp.concatenate(
        [first * cosine - second * sine, second * cosine + first * sine], axis=-1
    )


def moved_along_z(x, by):
    ring = lax.axis_size("gr") * lax.axis_size("sp") // Y
    pairs = [(z * Y + y, (z + by) % ring * Y + y) for z in range(ring) for y in range(Y)]
    return lax.ppermute(x, ("gr", "sp"), pairs)


def copies_along_y(arrays):
    groups = [[z * Y + y for y in range(Y)] for z in range(lax.axis_size("sp") // Y)]
    spread = [jnp.broadcast_to(x[None], (Y, *x.shape)) for x in arrays]
    spread = jnp.concatenate(spread, axis=-1)
    got = lax.all_to_all(spread, "sp", 0, 0, tiled=True, axis_index_groups=groups)
    return got.reshape(Y * got.shape[1], got.shape[2])


def projected(token_rows, arrays):
    planes = lax.axis_size("sp") // Y
    far = planes // 2
    mine = lax.axis_index("sp").astype(jnp.uint32) // Y
    block = copies_along_y(arrays)
    depth = block.shape[0]

    def part(weights, off):
        first = (mine + (off + planes)) % planes * depth
        cols = lax.dynamic_slice_in_dim(token_rows, first, depth, 1)
        return jnp.dot(cols, weights, preferred_element_type=jnp.float32)

    total = part(block, 0)
    up = down = block
    for hop in range(1, far):
        up, down = moved_along_z(up, 1), moved_along_z(down, -1)
        total += part(up, -hop) + part(down, hop)
    up, down = moved_along_z(up[: depth // 2], 1), moved_along_z(down[depth // 2 :], -1)
    return total + part(jnp.concatenate([up, down], axis=0), far)


def in_three(x):
    parts, rest = ([], x)
    for _ in range(PARTS):
        piece = lax.reduce_precision(rest, 8, 7)
        parts.append(piece.astype(jnp.bfloat16))
        rest = rest - piece
    return parts


def lanes_of(shape):
    return lax.broadcasted_iota(jnp.int32, shape, 1)


def rows_of(shape):
    return lax.broadcasted_iota(jnp.int32, shape, 0)


def share_kernel(seqs, sums_ref, cosine_ref, sine_ref, weight_ref, carried_ref, out_ref):
    cols = out_ref.shape[0]
    heads = cols // HEAD_DIM
    span = sums_ref.shape[0] // seqs
    half = HEAD_DIM // 2
    low = lanes_of((span, cols)) % HEAD_DIM < half
    spread = (rows_of((heads, cols)) == lanes_of((heads, cols)) // HEAD_DIM).astype(F32)
    blocks = [[] for _ in range(heads)]
    for seq in range(seqs):
        here = pl.ds(seq * span, span)
        keys = sums_ref[here, :cols].astype(BF16).astype(F32)
        values = sums_ref[here, cols:].astype(BF16)
        other = jnp.where(low, pltpu.roll(keys, cols - half, 1), pltpu.roll(keys, half, 1))
        turned = keys * cosine_ref[...] + other * sine_ref[...]
        faded = turned * jnp.dot(weight_ref[here, :], spread, precision=EXACT)
        high = faded.astype(BF16)
        rest = (faded - high.astype(F32)).astype(BF16)
        product = sum(
            lax.dot_general(
                values, part, (((0,), (0,)), ((), ())), preferred_element_type=F32
            )
            for part in (high, rest)
        )
        for head in range(heads):
            cut = slice(head * HEAD_DIM, (head + 1) * HEAD_DIM)
            blocks[head].append(product[cut, cut])
    for head in range(heads):
        cut = pl.ds(head * HEAD_DIM, HEAD_DIM)
        out_ref[cut, : seqs * HEAD_DIM] = jnp.concatenate(blocks[head], axis=1).astype(BF16)
    out_ref[:, seqs * HEAD_DIM :] = carried_ref[...]


def owner_kernel(devices, seqs, got_ref, lines_ref, values_ref, out_ref):
    total, lanes = (got_ref.shape[0], seqs * HEAD_DIM)
    rows = total // devices
    later = (lanes_of((devices, total)) // rows > rows_of((devices, total))) & (
        lanes_of((devices, total)) % rows == 0
    )
    sums = jnp.dot(later.astype(BF16), got_ref[:, lanes:], preferred_element_type=F32)
    place = (EXTRA, lanes)
    wide = (rows_of(place) // PARTS == lanes_of(place) // HEAD_DIM).astype(F32)
    fade = jnp.exp(jnp.dot(sums, wide, precision=EXACT))
    shares = got_ref[:, :lanes].astype(F32)
    owned = shares[:rows] * fade[0:1]
    for device in range(1, devices):
        owned += shares[device * rows : (device + 1) * rows] * fade[device : device + 1]
    finished = lines_ref[0:1] * owned + lines_ref[1:2] * values_ref[...]
    place = (lanes, EXTRA)
    fold = rows_of(place) // HEAD_DIM == lanes_of(place) % seqs
    read = jnp.dot(finished * lines_ref[2:3], fold.astype(F32), precision=EXACT)
    piece = lanes_of(read.shape) // seqs
    rest, packed = (read, jnp.zeros_like(read))
    for part in range(PARTS):
        rounded = rest.astype(BF16).astype(F32)
        packed = jnp.where(piece == part, rounded, packed)
        rest = rest - rounded
    line = jnp.concatenate([finished, packed], axis=1)
    out_ref[...] = jnp.concatenate([line] * devices, axis=0).astype(BF16)


def read_kernel(seqs, got_ref, gain_ref, state_ref, read_ref):
    cols, lanes = (got_ref.shape[0], seqs * HEAD_DIM)
    state_ref[...] = got_ref[:, :lanes].astype(F32)
    place = (8, EXTRA)
    pick = (lanes_of(place) % seqs == rows_of(place)) & (lanes_of(place) < seqs * PARTS)
    raw = lax.dot_general(
        pick.astype(BF16), got_ref[:, lanes:], (((1,), (1,)), ((), ())), preferred_element_type=F32
    )
    place = (cols, cols)
    mean = (rows_of(place) // HEAD_DIM == lanes_of(place) // HEAD_DIM).astype(F32) / HEAD_DIM
    center = raw - jnp.dot(raw, mean, precision=EXACT)
    spread = jnp.dot(center * center, mean, precision=EXACT)
    normed = center * lax.rsqrt(spread + 1e-06) * gain_ref[...]
    read_ref[...] = normed[:seqs].astype(BF16)


def in_vmem(kernel, shapes, *operands):
    space = pl.BlockSpec(memory_space=pltpu.VMEM)
    many = isinstance(shapes, list)
    return pl.pallas_call(
        kernel,
        out_shape=shapes,
        in_specs=[space] * len(operands),
        out_specs=[space] * len(shapes) if many else space,
        compiler_params=pltpu.CompilerParams(vmem_limit_bytes=16 * 2**20),
    )(*operands)


def shards(
    tokens,
    key_weight,
    value_weight,
    log_decay,
    new_query,
    new_key,
    new_value,
    step_decay,
    norm_gain,
):
    seqs, span, width = tokens.shape
    heads = key_weight.shape[1] // HEAD_DIM
    cols = heads * HEAD_DIM
    lanes = seqs * HEAD_DIM
    half = HEAD_DIM // 2
    devices, mine = (lax.axis_size("sp"), lax.axis_index("sp"))
    rows = cols // devices

    positions = (mine * span + jnp.arange(span, dtype=jnp.int32)).astype(F32)
    inverse = 10000.0 ** (-jnp.arange(half, dtype=F32) * (2.0 / HEAD_DIM))
    angles = positions[:, None] * inverse
    cosine = jnp.tile(jnp.cos(angles), (1, 2 * heads)) * HEAD_DIM ** (-0.5)
    sine = jnp.sin(angles) * HEAD_DIM ** (-0.5)
    sine = jnp.tile(jnp.concatenate([-sine, sine], axis=1), (1, heads))
    totals = jnp.sum(log_decay, axis=-1)
    weight = jnp.exp(totals[:, :, None] - jnp.cumsum(log_decay, axis=-1))
    weight = jnp.transpose(weight, (1, 2, 0)).reshape(seqs * span, heads)
    carried = jnp.stack(in_three(totals), axis=-1).reshape(heads, 1, 1, seqs * PARTS)
    carried = jnp.broadcast_to(carried, (heads, devices // heads, 1, seqs * PARTS))
    carried = carried.reshape(devices, 1, seqs * PARTS)
    carried = jnp.pad(carried, ((0, 0), (0, rows - 1), (0, EXTRA - seqs * PARTS)))
    carried = carried.reshape(cols, EXTRA)

    end_pos = jnp.full((seqs, heads), float(span * devices), F32)
    query = rotate_half(new_query.astype(F32).reshape(seqs, heads, HEAD_DIM), end_pos)
    key_new = rotate_half(
        new_key.astype(F32).reshape(seqs, heads, HEAD_DIM), end_pos
    ) * HEAD_DIM ** (-0.5)
    decay_lanes = jnp.repeat(jnp.exp(step_decay), HEAD_DIM, axis=1)
    by_head = [jnp.transpose(x, (1, 0, 2)).reshape(heads, lanes) for x in (key_new, query)]
    lines = jnp.stack([decay_lanes, *by_head], axis=1)
    lines = lax.dynamic_index_in_dim(lines, mine // (devices // heads), 0, keepdims=False)
    value_cols = jnp.repeat(new_value.astype(F32).T, HEAD_DIM, axis=1)
    value_rows = lax.dynamic_slice_in_dim(value_cols, mine * rows, rows, 0)
    ready = lax.optimization_barrier((cosine, sine, weight, carried, lines, value_rows))
    cosine, sine, weight, carried, lines, value_rows = ready

    sums = projected(tokens.reshape(seqs * span, width), (key_weight, value_weight))
    whole = jax.ShapeDtypeStruct((cols, lanes + EXTRA), BF16)

    def exchanged(x):
        cut = x.reshape(devices, rows, lanes + EXTRA)
        return lax.all_to_all(cut, "sp", 0, 0, tiled=True).reshape(x.shape)

    sent = in_vmem(
        functools.partial(share_kernel, seqs), whole, sums, cosine, sine, weight, carried
    )
    finished = in_vmem(
        functools.partial(owner_kernel, devices, seqs), whole, exchanged(sent), lines, value_rows
    )
    state, first_read = in_vmem(
        functools.partial(read_kernel, seqs),
        [jax.ShapeDtypeStruct((cols, lanes), F32), jax.ShapeDtypeStruct((seqs, cols), BF16)],
        exchanged(finished),
        norm_gain.reshape(1, cols),
    )
    state_cache = jnp.transpose(state.reshape(heads, HEAD_DIM, lanes), (2, 0, 1))
    return (state_cache, first_read)


def solution(mesh):
    placed = (
        P("gr", "sp", None),
        P("sp", "tp"),
        P("sp", "tp"),
        P("tp", "gr", "sp"),
        P("gr", "tp"),
        P("gr", "tp"),
        P("gr", "tp"),
        P("tp", "gr"),
        P("tp"),
    )
    return jax.shard_map(
        shards,
        mesh=mesh,
        in_specs=placed,
        out_specs=(P("gr", "tp", None), P("gr", "tp")),
        check_vma=False,
    )
```

```python
import functools

import jax
import jax.numpy as jnp
from jax import lax
from jax.experimental import pallas as pl
from jax.experimental.pallas import tpu as pltpu
from jax.sharding import PartitionSpec as P

HEAD_DIM = 64
Y = 4
PARTS = 3
EXTRA = 128
EXACT = lax.Precision.HIGHEST
F32, BF16 = (jnp.float32, jnp.bfloat16)


def rotate_half(values, positions):
    half = values.shape[-1] // 2
    inverse = 10000.0 ** (-jnp.arange(half, dtype=jnp.float32) * (2.0 / values.shape[-1]))
    angles = positions[..., None] * inverse
    cosine = jnp.cos(angles)
    sine = jnp.sin(angles)
    first, second = (values[..., :half], values[..., half:])
    return jnp.concatenate(
        [first * cosine - second * sine, second * cosine + first * sine], axis=-1
    )


def moved_along_z(x, by):
    ring = lax.axis_size("gr") * lax.axis_size("sp") // Y
    pairs = [(z * Y + y, (z + by) % ring * Y + y) for z in range(ring) for y in range(Y)]
    return lax.ppermute(x, ("gr", "sp"), pairs)


def from_opposite_plane(x):
    ring = lax.axis_size("gr") * lax.axis_size("sp") // Y
    wide = lax.axis_size("tp")
    far = lax.axis_size("sp") // Y // 2
    pairs = []
    for z in range(ring):
        for y in range(Y):
            for t in range(wide):
                to = (z + (far if t % 2 else -far)) % ring
                pairs.append(((z * Y + y) * wide + t, (to * Y + y) * wide + t))
    return lax.ppermute(x, ("gr", "sp", "tp"), pairs)


def copies_along_y(x):
    groups = [[z * Y + y for y in range(Y)] for z in range(lax.axis_size("sp") // Y)]
    spread = jnp.broadcast_to(x[None], (Y, *x.shape))
    got = lax.all_to_all(spread, "sp", 0, 0, tiled=True, axis_index_groups=groups)
    return got.reshape(Y * got.shape[1], got.shape[2])


def projected(token_rows, own):
    planes = lax.axis_size("sp") // Y
    far = planes // 2
    mine = lax.axis_index("sp").astype(jnp.uint32) // Y
    block = copies_along_y(own)
    opposite = from_opposite_plane(own)
    depth = block.shape[0]

    def part(weights, off):
        first = (mine + (off + planes)) % planes * depth
        cols = lax.dynamic_slice_in_dim(token_rows, first, depth, 1)
        return jnp.dot(cols, weights, preferred_element_type=jnp.float32)

    total = part(block, 0)
    down = moved_along_z(block, -1)
    up = moved_along_z(block, 1)
    spread = copies_along_y(opposite)
    for hop in range(1, far):
        total += part(up, -hop) + part(down, hop)
        if hop + 1 < far:
            up, down = moved_along_z(up, 1), moved_along_z(down, -1)
        if hop == 1:
            total, spread = lax.optimization_barrier((total, spread))
            total += part(spread, far)
    return total


def in_three(x):
    parts, rest = ([], x)
    for _ in range(PARTS):
        piece = lax.reduce_precision(rest, 8, 7)
        parts.append(piece.astype(jnp.bfloat16))
        rest = rest - piece
    return parts


def lanes_of(shape):
    return lax.broadcasted_iota(jnp.int32, shape, 1)


def rows_of(shape):
    return lax.broadcasted_iota(jnp.int32, shape, 0)


def share_kernel(seqs, sums_ref, cosine_ref, sine_ref, weight_ref, carried_ref, out_ref):
    cols = out_ref.shape[0]
    heads = cols // HEAD_DIM
    span = sums_ref.shape[0] // seqs
    half = HEAD_DIM // 2
    low = lanes_of((span, cols)) % HEAD_DIM < half
    spread = (rows_of((heads, cols)) == lanes_of((heads, cols)) // HEAD_DIM).astype(F32)
    blocks = [[] for _ in range(heads)]
    for seq in range(seqs):
        here = pl.ds(seq * span, span)
        keys = sums_ref[here, :cols].astype(BF16).astype(F32)
        values = sums_ref[here, cols:].astype(BF16)
        other = jnp.where(low, pltpu.roll(keys, cols - half, 1), pltpu.roll(keys, half, 1))
        turned = keys * cosine_ref[...] + other * sine_ref[...]
        faded = turned * jnp.dot(weight_ref[here, :], spread, precision=EXACT)
        high = faded.astype(BF16)
        rest = (faded - high.astype(F32)).astype(BF16)
        product = sum(
            lax.dot_general(
                values, part, (((0,), (0,)), ((), ())), preferred_element_type=F32
            )
            for part in (high, rest)
        )
        for head in range(heads):
            cut = slice(head * HEAD_DIM, (head + 1) * HEAD_DIM)
            blocks[head].append(product[cut, cut])
    for head in range(heads):
        cut = pl.ds(head * HEAD_DIM, HEAD_DIM)
        out_ref[cut, : seqs * HEAD_DIM] = jnp.concatenate(blocks[head], axis=1).astype(BF16)
    out_ref[:, seqs * HEAD_DIM :] = carried_ref[...]


def owner_kernel(devices, seqs, got_ref, lines_ref, values_ref, out_ref):
    total, lanes = (got_ref.shape[0], seqs * HEAD_DIM)
    rows = total // devices
    later = (lanes_of((devices, total)) // rows > rows_of((devices, total))) & (
        lanes_of((devices, total)) % rows == 0
    )
    sums = jnp.dot(later.astype(BF16), got_ref[:, lanes:], preferred_element_type=F32)
    place = (EXTRA, lanes)
    wide = (rows_of(place) // PARTS == lanes_of(place) // HEAD_DIM).astype(F32)
    fade = jnp.exp(jnp.dot(sums, wide, precision=EXACT))
    shares = got_ref[:, :lanes].astype(F32)
    owned = shares[:rows] * fade[0:1]
    for device in range(1, devices):
        owned += shares[device * rows : (device + 1) * rows] * fade[device : device + 1]
    finished = lines_ref[0:1] * owned + lines_ref[1:2] * values_ref[...]
    place = (lanes, EXTRA)
    fold = rows_of(place) // HEAD_DIM == lanes_of(place) % seqs
    read = jnp.dot(finished * lines_ref[2:3], fold.astype(F32), precision=EXACT)
    piece = lanes_of(read.shape) // seqs
    rest, packed = (read, jnp.zeros_like(read))
    for part in range(PARTS):
        rounded = rest.astype(BF16).astype(F32)
        packed = jnp.where(piece == part, rounded, packed)
        rest = rest - rounded
    line = jnp.concatenate([finished, packed], axis=1)
    out_ref[...] = jnp.concatenate([line] * devices, axis=0).astype(BF16)


def read_kernel(seqs, got_ref, gain_ref, state_ref, read_ref):
    cols, lanes = (got_ref.shape[0], seqs * HEAD_DIM)
    state_ref[...] = got_ref[:, :lanes].astype(F32)
    place = (8, EXTRA)
    pick = (lanes_of(place) % seqs == rows_of(place)) & (lanes_of(place) < seqs * PARTS)
    raw = lax.dot_general(
        pick.astype(BF16), got_ref[:, lanes:], (((1,), (1,)), ((), ())), preferred_element_type=F32
    )
    place = (cols, cols)
    mean = (rows_of(place) // HEAD_DIM == lanes_of(place) // HEAD_DIM).astype(F32) / HEAD_DIM
    center = raw - jnp.dot(raw, mean, precision=EXACT)
    spread = jnp.dot(center * center, mean, precision=EXACT)
    normed = center * lax.rsqrt(spread + 1e-06) * gain_ref[...]
    read_ref[...] = normed[:seqs].astype(BF16)


def in_vmem(kernel, shapes, *operands):
    space = pl.BlockSpec(memory_space=pltpu.VMEM)
    many = isinstance(shapes, list)
    return pl.pallas_call(
        kernel,
        out_shape=shapes,
        in_specs=[space] * len(operands),
        out_specs=[space] * len(shapes) if many else space,
        compiler_params=pltpu.CompilerParams(vmem_limit_bytes=16 * 2**20),
    )(*operands)


def shards(
    tokens,
    key_weight,
    value_weight,
    log_decay,
    new_query,
    new_key,
    new_value,
    step_decay,
    norm_gain,
):
    seqs, span, width = tokens.shape
    heads = key_weight.shape[1] // HEAD_DIM
    cols = heads * HEAD_DIM
    lanes = seqs * HEAD_DIM
    half = HEAD_DIM // 2
    devices, mine = (lax.axis_size("sp"), lax.axis_index("sp"))
    rows = cols // devices

    positions = (mine * span + jnp.arange(span, dtype=jnp.int32)).astype(F32)
    inverse = 10000.0 ** (-jnp.arange(half, dtype=F32) * (2.0 / HEAD_DIM))
    angles = positions[:, None] * inverse
    cosine = jnp.tile(jnp.cos(angles), (1, 2 * heads)) * HEAD_DIM ** (-0.5)
    sine = jnp.sin(angles) * HEAD_DIM ** (-0.5)
    sine = jnp.tile(jnp.concatenate([-sine, sine], axis=1), (1, heads))
    totals = jnp.sum(log_decay, axis=-1)
    weight = jnp.exp(totals[:, :, None] - jnp.cumsum(log_decay, axis=-1))
    weight = jnp.transpose(weight, (1, 2, 0)).reshape(seqs * span, heads)
    carried = jnp.stack(in_three(totals), axis=-1).reshape(heads, 1, 1, seqs * PARTS)
    carried = jnp.broadcast_to(carried, (heads, devices // heads, 1, seqs * PARTS))
    carried = carried.reshape(devices, 1, seqs * PARTS)
    carried = jnp.pad(carried, ((0, 0), (0, rows - 1), (0, EXTRA - seqs * PARTS)))
    carried = carried.reshape(cols, EXTRA)

    end_pos = jnp.full((seqs, heads), float(span * devices), F32)
    query = rotate_half(new_query.astype(F32).reshape(seqs, heads, HEAD_DIM), end_pos)
    key_new = rotate_half(
        new_key.astype(F32).reshape(seqs, heads, HEAD_DIM), end_pos
    ) * HEAD_DIM ** (-0.5)
    decay_lanes = jnp.repeat(jnp.exp(step_decay), HEAD_DIM, axis=1)
    by_head = [jnp.transpose(x, (1, 0, 2)).reshape(heads, lanes) for x in (key_new, query)]
    lines = jnp.stack([decay_lanes, *by_head], axis=1)
    lines = lax.dynamic_index_in_dim(lines, mine // (devices // heads), 0, keepdims=False)
    value_cols = jnp.repeat(new_value.astype(F32).T, HEAD_DIM, axis=1)
    value_rows = lax.dynamic_slice_in_dim(value_cols, mine * rows, rows, 0)
    ready = lax.optimization_barrier((cosine, sine, weight, carried, lines, value_rows))
    cosine, sine, weight, carried, lines, value_rows = ready

    own = jnp.concatenate([key_weight, value_weight], axis=1)
    sums = projected(tokens.reshape(seqs * span, width), own)
    whole = jax.ShapeDtypeStruct((cols, lanes + EXTRA), BF16)

    def exchanged(x):
        cut = x.reshape(devices, rows, lanes + EXTRA)
        return lax.all_to_all(cut, "sp", 0, 0, tiled=True).reshape(x.shape)

    sent = in_vmem(
        functools.partial(share_kernel, seqs), whole, sums, cosine, sine, weight, carried
    )
    finished = in_vmem(
        functools.partial(owner_kernel, devices, seqs), whole, exchanged(sent), lines, value_rows
    )
    state, first_read = in_vmem(
        functools.partial(read_kernel, seqs),
        [jax.ShapeDtypeStruct((cols, lanes), F32), jax.ShapeDtypeStruct((seqs, cols), BF16)],
        exchanged(finished),
        norm_gain.reshape(1, cols),
    )
    state_cache = jnp.transpose(state.reshape(heads, HEAD_DIM, lanes), (2, 0, 1))
    return (state_cache, first_read)


def solution(mesh):
    placed = (
        P("gr", "sp", None),
        P("sp", "tp"),
        P("sp", "tp"),
        P("tp", "gr", "sp"),
        P("gr", "tp"),
        P("gr", "tp"),
        P("gr", "tp"),
        P("tp", "gr"),
        P("tp"),
    )
    return jax.shard_map(
        shards,
        mesh=mesh,
        in_specs=placed,
        out_specs=(P("gr", "tp", None), P("gr", "tp")),
        check_vma=False,
    )
```

```python
import functools

import jax
import jax.numpy as jnp
from jax import lax
from jax.experimental import pallas as pl
from jax.experimental.pallas import tpu as pltpu
from jax.sharding import PartitionSpec as P

HEAD_DIM = 64
Y = 4
PARTS = 3
EXTRA = 128
EXACT = lax.Precision.HIGHEST
F32, BF16 = (jnp.float32, jnp.bfloat16)


def rotate_half(values, positions):
    half = values.shape[-1] // 2
    inverse = 10000.0 ** (-jnp.arange(half, dtype=jnp.float32) * (2.0 / values.shape[-1]))
    angles = positions[..., None] * inverse
    cosine = jnp.cos(angles)
    sine = jnp.sin(angles)
    first, second = (values[..., :half], values[..., half:])
    return jnp.concatenate(
        [first * cosine - second * sine, second * cosine + first * sine], axis=-1
    )


def moved_along_z(x, by):
    ring = lax.axis_size("gr") * lax.axis_size("sp") // Y
    pairs = [(z * Y + y, (z + by) % ring * Y + y) for z in range(ring) for y in range(Y)]
    return lax.ppermute(x, ("gr", "sp"), pairs)


def from_opposite_plane(x):
    ring = lax.axis_size("gr") * lax.axis_size("sp") // Y
    wide = lax.axis_size("tp")
    far = lax.axis_size("sp") // Y // 2
    pairs = []
    for z in range(ring):
        for y in range(Y):
            for t in range(wide):
                to = (z + (far if t % 2 else -far)) % ring
                pairs.append(((z * Y + y) * wide + t, (to * Y + y) * wide + t))
    return lax.ppermute(x, ("gr", "sp", "tp"), pairs)


def exchanged_along_y(spread):
    groups = [[z * Y + y for y in range(Y)] for z in range(lax.axis_size("sp") // Y)]
    got = lax.all_to_all(spread, "sp", 0, 0, tiled=True, axis_index_groups=groups)
    return got.reshape(Y * got.shape[1], got.shape[2])


def projected(token_rows, own, spread):
    planes = lax.axis_size("sp") // Y
    far = planes // 2
    mine = lax.axis_index("sp").astype(jnp.uint32) // Y
    block = exchanged_along_y(spread)
    opposite = from_opposite_plane(own)
    depth = block.shape[0]

    def part(weights, off):
        first = (mine + (off + planes)) % planes * depth
        cols = lax.dynamic_slice_in_dim(token_rows, first, depth, 1)
        return jnp.dot(cols, weights, preferred_element_type=F32)

    total = part(block, 0)
    up = down = block
    for hop in range(1, far):
        down = moved_along_z(down, -1)
        up = moved_along_z(up, 1)
        if hop + 1 < far:
            total += part(up, -hop) + part(down, hop)
    distant = exchanged_along_y(jnp.broadcast_to(opposite[None], (Y, *opposite.shape)))
    total += part(distant, far)
    return total + part(up, 1 - far) + part(down, far - 1)


def in_three(x):
    parts, rest = ([], x)
    for _ in range(PARTS):
        piece = lax.reduce_precision(rest, 8, 7)
        parts.append(piece.astype(jnp.bfloat16))
        rest = rest - piece
    return parts


def lanes_of(shape):
    return lax.broadcasted_iota(jnp.int32, shape, 1)


def rows_of(shape):
    return lax.broadcasted_iota(jnp.int32, shape, 0)


def spread_kernel(key_ref, value_ref, own_ref, spread_ref):
    both = jnp.concatenate([key_ref[...], value_ref[...]], axis=1)
    own_ref[...] = both
    for y in range(Y):
        spread_ref[y] = both


def share_kernel(seqs, sums_ref, cosine_ref, sine_ref, weight_ref, carried_ref, out_ref):
    cols = out_ref.shape[0]
    heads = cols // HEAD_DIM
    span = sums_ref.shape[0] // seqs
    half = HEAD_DIM // 2
    low = lanes_of((span, cols)) % HEAD_DIM < half
    spread = (rows_of((heads, cols)) == lanes_of((heads, cols)) // HEAD_DIM).astype(F32)
    blocks = [[] for _ in range(heads)]
    for seq in range(seqs):
        here = pl.ds(seq * span, span)
        keys = sums_ref[here, :cols].astype(BF16).astype(F32)
        values = sums_ref[here, cols:].astype(BF16)
        other = jnp.where(low, pltpu.roll(keys, cols - half, 1), pltpu.roll(keys, half, 1))
        turned = keys * cosine_ref[...] + other * sine_ref[...]
        faded = turned * jnp.dot(weight_ref[here, :], spread, precision=EXACT)
        high = faded.astype(BF16)
        rest = (faded - high.astype(F32)).astype(BF16)
        product = sum(
            lax.dot_general(
                values, part, (((0,), (0,)), ((), ())), preferred_element_type=F32
            )
            for part in (high, rest)
        )
        for head in range(heads):
            cut = slice(head * HEAD_DIM, (head + 1) * HEAD_DIM)
            blocks[head].append(product[cut, cut])
    for head in range(heads):
        cut = pl.ds(head * HEAD_DIM, HEAD_DIM)
        out_ref[cut, : seqs * HEAD_DIM] = jnp.concatenate(blocks[head], axis=1).astype(BF16)
    out_ref[:, seqs * HEAD_DIM :] = carried_ref[...]


def owner_kernel(devices, seqs, got_ref, lines_ref, values_ref, out_ref):
    total, lanes = (got_ref.shape[0], seqs * HEAD_DIM)
    rows = total // devices
    later = (lanes_of((devices, total)) // rows > rows_of((devices, total))) & (
        lanes_of((devices, total)) % rows == 0
    )
    sums = jnp.dot(later.astype(BF16), got_ref[:, lanes:], preferred_element_type=F32)
    place = (EXTRA, lanes)
    wide = (rows_of(place) // PARTS == lanes_of(place) // HEAD_DIM).astype(F32)
    fade = jnp.exp(jnp.dot(sums, wide, precision=EXACT))
    shares = got_ref[:, :lanes].astype(F32)
    owned = shares[:rows] * fade[0:1]
    for device in range(1, devices):
        owned += shares[device * rows : (device + 1) * rows] * fade[device : device + 1]
    finished = lines_ref[0:1] * owned + lines_ref[1:2] * values_ref[...]
    place = (lanes, EXTRA)
    fold = rows_of(place) // HEAD_DIM == lanes_of(place) % seqs
    read = jnp.dot(finished * lines_ref[2:3], fold.astype(F32), precision=EXACT)
    piece = lanes_of(read.shape) // seqs
    rest, packed = (read, jnp.zeros_like(read))
    for part in range(PARTS):
        rounded = rest.astype(BF16).astype(F32)
        packed = jnp.where(piece == part, rounded, packed)
        rest = rest - rounded
    line = jnp.concatenate([finished, packed], axis=1)
    out_ref[...] = jnp.concatenate([line] * devices, axis=0).astype(BF16)


def read_kernel(seqs, got_ref, gain_ref, state_ref, read_ref):
    cols, lanes = (got_ref.shape[0], seqs * HEAD_DIM)
    state_ref[...] = got_ref[:, :lanes].astype(F32)
    place = (8, EXTRA)
    pick = (lanes_of(place) % seqs == rows_of(place)) & (lanes_of(place) < seqs * PARTS)
    raw = lax.dot_general(
        pick.astype(BF16), got_ref[:, lanes:], (((1,), (1,)), ((), ())), preferred_element_type=F32
    )
    place = (cols, cols)
    mean = (rows_of(place) // HEAD_DIM == lanes_of(place) // HEAD_DIM).astype(F32) / HEAD_DIM
    center = raw - jnp.dot(raw, mean, precision=EXACT)
    spread = jnp.dot(center * center, mean, precision=EXACT)
    normed = center * lax.rsqrt(spread + 1e-06) * gain_ref[...]
    read_ref[...] = normed[:seqs].astype(BF16)


def in_vmem(kernel, shapes, *operands):
    space = pl.BlockSpec(memory_space=pltpu.VMEM)
    many = isinstance(shapes, list)
    return pl.pallas_call(
        kernel,
        out_shape=shapes,
        in_specs=[space] * len(operands),
        out_specs=[space] * len(shapes) if many else space,
        compiler_params=pltpu.CompilerParams(vmem_limit_bytes=16 * 2**20),
    )(*operands)


def shards(
    tokens,
    key_weight,
    value_weight,
    log_decay,
    new_query,
    new_key,
    new_value,
    step_decay,
    norm_gain,
):
    seqs, span, width = tokens.shape
    heads = key_weight.shape[1] // HEAD_DIM
    cols = heads * HEAD_DIM
    lanes = seqs * HEAD_DIM
    half = HEAD_DIM // 2
    devices, mine = (lax.axis_size("sp"), lax.axis_index("sp"))
    rows = cols // devices

    positions = (mine * span + jnp.arange(span, dtype=jnp.int32)).astype(F32)
    inverse = 10000.0 ** (-jnp.arange(half, dtype=F32) * (2.0 / HEAD_DIM))
    angles = positions[:, None] * inverse
    cosine = jnp.tile(jnp.cos(angles), (1, 2 * heads)) * HEAD_DIM ** (-0.5)
    sine = jnp.sin(angles) * HEAD_DIM ** (-0.5)
    sine = jnp.tile(jnp.concatenate([-sine, sine], axis=1), (1, heads))
    totals = jnp.sum(log_decay, axis=-1)
    weight = jnp.exp(totals[:, :, None] - jnp.cumsum(log_decay, axis=-1))
    weight = jnp.transpose(weight, (1, 2, 0)).reshape(seqs * span, heads)
    carried = jnp.stack(in_three(totals), axis=-1).reshape(heads, 1, 1, seqs * PARTS)
    carried = jnp.broadcast_to(carried, (heads, devices // heads, 1, seqs * PARTS))
    carried = carried.reshape(devices, 1, seqs * PARTS)
    carried = jnp.pad(carried, ((0, 0), (0, rows - 1), (0, EXTRA - seqs * PARTS)))
    carried = carried.reshape(cols, EXTRA)

    end_pos = jnp.full((seqs, heads), float(span * devices), F32)
    query = rotate_half(new_query.astype(F32).reshape(seqs, heads, HEAD_DIM), end_pos)
    key_new = rotate_half(
        new_key.astype(F32).reshape(seqs, heads, HEAD_DIM), end_pos
    ) * HEAD_DIM ** (-0.5)
    decay_lanes = jnp.repeat(jnp.exp(step_decay), HEAD_DIM, axis=1)
    by_head = [jnp.transpose(x, (1, 0, 2)).reshape(heads, lanes) for x in (key_new, query)]
    lines = jnp.stack([decay_lanes, *by_head], axis=1)
    lines = lax.dynamic_index_in_dim(lines, mine // (devices // heads), 0, keepdims=False)
    value_cols = jnp.repeat(new_value.astype(F32).T, HEAD_DIM, axis=1)
    value_rows = lax.dynamic_slice_in_dim(value_cols, mine * rows, rows, 0)
    ready = lax.optimization_barrier((cosine, sine, weight, carried))
    cosine, sine, weight, carried = ready

    depth = key_weight.shape[0]
    own, spread = in_vmem(
        spread_kernel,
        [
            jax.ShapeDtypeStruct((depth, 2 * cols), BF16),
            jax.ShapeDtypeStruct((Y, depth, 2 * cols), BF16),
        ],
        key_weight,
        value_weight,
    )
    sums = projected(tokens.reshape(seqs * span, width), own, spread)
    whole = jax.ShapeDtypeStruct((cols, lanes + EXTRA), BF16)

    def exchanged(x):
        cut = x.reshape(devices, rows, lanes + EXTRA)
        return lax.all_to_all(cut, "sp", 0, 0, tiled=True).reshape(x.shape)

    sent = in_vmem(
        functools.partial(share_kernel, seqs), whole, sums, cosine, sine, weight, carried
    )
    finished = in_vmem(
        functools.partial(owner_kernel, devices, seqs), whole, exchanged(sent), lines, value_rows
    )
    state, first_read = in_vmem(
        functools.partial(read_kernel, seqs),
        [jax.ShapeDtypeStruct((cols, lanes), F32), jax.ShapeDtypeStruct((seqs, cols), BF16)],
        exchanged(finished),
        norm_gain.reshape(1, cols),
    )
    state_cache = jnp.transpose(state.reshape(heads, HEAD_DIM, lanes), (2, 0, 1))
    return (state_cache, first_read)


def solution(mesh):
    placed = (
        P("gr", "sp", None),
        P("sp", "tp"),
        P("sp", "tp"),
        P("tp", "gr", "sp"),
        P("gr", "tp"),
        P("gr", "tp"),
        P("gr", "tp"),
        P("tp", "gr"),
        P("tp"),
    )
    return jax.shard_map(
        shards,
        mesh=mesh,
        in_specs=placed,
        out_specs=(P("gr", "tp", None), P("gr", "tp")),
        check_vma=False,
    )
```

```python
import functools

import jax
import jax.numpy as jnp
from jax import lax
from jax.experimental import pallas as pl
from jax.experimental.pallas import tpu as pltpu
from jax.sharding import PartitionSpec as P

HEAD_DIM = 64
Y = 4
PARTS = 3
EXTRA = 128
EXACT = lax.Precision.HIGHEST
F32, BF16 = (jnp.float32, jnp.bfloat16)


def rotate_half(values, positions):
    half = values.shape[-1] // 2
    inverse = 10000.0 ** (-jnp.arange(half, dtype=jnp.float32) * (2.0 / values.shape[-1]))
    angles = positions[..., None] * inverse
    cosine = jnp.cos(angles)
    sine = jnp.sin(angles)
    first, second = (values[..., :half], values[..., half:])
    return jnp.concatenate(
        [first * cosine - second * sine, second * cosine + first * sine], axis=-1
    )


def moved_along_z(x, by):
    ring = lax.axis_size("gr") * lax.axis_size("sp") // Y
    pairs = [(z * Y + y, (z + by) % ring * Y + y) for z in range(ring) for y in range(Y)]
    return lax.ppermute(x, ("gr", "sp"), pairs)


def from_opposite_plane(x):
    ring = lax.axis_size("gr") * lax.axis_size("sp") // Y
    wide = lax.axis_size("tp")
    far = lax.axis_size("sp") // Y // 2
    pairs = []
    for z in range(ring):
        for y in range(Y):
            for t in range(wide):
                to = (z + (far if t % 2 else -far)) % ring
                pairs.append(((z * Y + y) * wide + t, (to * Y + y) * wide + t))
    return lax.ppermute(x, ("gr", "sp", "tp"), pairs)


def moved_along_y(x, by):
    planes = lax.axis_size("sp") // Y
    pairs = [(z * Y + y, z * Y + (y + by) % Y) for z in range(planes) for y in range(Y)]
    return lax.ppermute(x, "sp", pairs)


def exchanged_along_y(spread):
    groups = [[z * Y + y for y in range(Y)] for z in range(lax.axis_size("sp") // Y)]
    got = lax.all_to_all(spread, "sp", 0, 0, tiled=True, axis_index_groups=groups)
    return got.reshape(Y * got.shape[1], got.shape[2])


def projected(token_rows, own, spread):
    planes = lax.axis_size("sp") // Y
    far = planes // 2
    mine = lax.axis_index("sp").astype(jnp.uint32) // Y
    block = exchanged_along_y(spread)
    opposite = from_opposite_plane(own)
    depth = block.shape[0]
    row = lax.axis_index("sp").astype(jnp.uint32) % Y

    def part(weights, off, start=0):
        first = (mine + (off + planes)) % planes * depth + start
        cols = lax.dynamic_slice_in_dim(token_rows, first, weights.shape[0], 1)
        return jnp.dot(cols, weights, preferred_element_type=F32)

    def far_part(weights, by):
        return part(weights, far, (row + (Y - by)) % Y * own.shape[0])

    total = part(block, 0)
    up = down = block
    for hop in range(1, far):
        down = moved_along_z(down, -1)
        up = moved_along_z(up, 1)
        beside = moved_along_y(opposite, hop)
        if hop == 1:
            total += far_part(opposite, 0)
        total += far_part(beside, hop) + part(up, -hop) + part(down, hop)
    return total


def in_three(x):
    parts, rest = ([], x)
    for _ in range(PARTS):
        piece = lax.reduce_precision(rest, 8, 7)
        parts.append(piece.astype(jnp.bfloat16))
        rest = rest - piece
    return parts


def lanes_of(shape):
    return lax.broadcasted_iota(jnp.int32, shape, 1)


def rows_of(shape):
    return lax.broadcasted_iota(jnp.int32, shape, 0)


def spread_kernel(key_ref, value_ref, own_ref, spread_ref, sems):
    cols = key_ref.shape[1]
    copies = []
    for ref, cut in ((key_ref, pl.ds(0, cols)), (value_ref, pl.ds(cols, cols))):
        for to in (own_ref.at[:, cut], *(spread_ref.at[y, :, cut] for y in range(Y))):
            copies.append(pltpu.make_async_copy(ref, to, sems.at[len(copies)]))
    for copy in copies:
        copy.start()
    for copy in copies:
        copy.wait()


def share_kernel(seqs, sums_ref, cosine_ref, sine_ref, weight_ref, carried_ref, out_ref):
    cols = out_ref.shape[0]
    heads = cols // HEAD_DIM
    span = sums_ref.shape[0] // seqs
    half = HEAD_DIM // 2
    low = lanes_of((span, cols)) % HEAD_DIM < half
    spread = (rows_of((heads, cols)) == lanes_of((heads, cols)) // HEAD_DIM).astype(F32)
    blocks = [[] for _ in range(heads)]
    for seq in range(seqs):
        here = pl.ds(seq * span, span)
        keys = sums_ref[here, :cols].astype(BF16).astype(F32)
        values = sums_ref[here, cols:].astype(BF16)
        other = jnp.where(low, pltpu.roll(keys, cols - half, 1), pltpu.roll(keys, half, 1))
        turned = keys * cosine_ref[...] + other * sine_ref[...]
        faded = turned * jnp.dot(weight_ref[here, :], spread, precision=EXACT)
        high = faded.astype(BF16)
        rest = (faded - high.astype(F32)).astype(BF16)
        product = sum(
            lax.dot_general(
                values, part, (((0,), (0,)), ((), ())), preferred_element_type=F32
            )
            for part in (high, rest)
        )
        for head in range(heads):
            cut = slice(head * HEAD_DIM, (head + 1) * HEAD_DIM)
            blocks[head].append(product[cut, cut])
    for head in range(heads):
        cut = pl.ds(head * HEAD_DIM, HEAD_DIM)
        out_ref[cut, : seqs * HEAD_DIM] = jnp.concatenate(blocks[head], axis=1).astype(BF16)
    out_ref[:, seqs * HEAD_DIM :] = carried_ref[...]


def owner_kernel(devices, seqs, got_ref, lines_ref, values_ref, out_ref):
    total, lanes = (got_ref.shape[0], seqs * HEAD_DIM)
    rows = total // devices
    later = (lanes_of((devices, total)) // rows > rows_of((devices, total))) & (
        lanes_of((devices, total)) % rows == 0
    )
    sums = jnp.dot(later.astype(BF16), got_ref[:, lanes:], preferred_element_type=F32)
    place = (EXTRA, lanes)
    wide = (rows_of(place) // PARTS == lanes_of(place) // HEAD_DIM).astype(F32)
    fade = jnp.exp(jnp.dot(sums, wide, precision=EXACT))
    shares = got_ref[:, :lanes].astype(F32)
    owned = shares[:rows] * fade[0:1]
    for device in range(1, devices):
        owned += shares[device * rows : (device + 1) * rows] * fade[device : device + 1]
    finished = lines_ref[0:1] * owned + lines_ref[1:2] * values_ref[...]
    place = (lanes, EXTRA)
    fold = rows_of(place) // HEAD_DIM == lanes_of(place) % seqs
    read = jnp.dot(finished * lines_ref[2:3], fold.astype(F32), precision=EXACT)
    piece = lanes_of(read.shape) // seqs
    rest, packed = (read, jnp.zeros_like(read))
    for part in range(PARTS):
        rounded = rest.astype(BF16).astype(F32)
        packed = jnp.where(piece == part, rounded, packed)
        rest = rest - rounded
    line = jnp.concatenate([finished, packed], axis=1)
    out_ref[...] = jnp.concatenate([line] * devices, axis=0).astype(BF16)


def read_kernel(seqs, got_ref, gain_ref, state_ref, read_ref):
    cols, lanes = (got_ref.shape[0], seqs * HEAD_DIM)
    state_ref[...] = got_ref[:, :lanes].astype(F32)
    place = (8, EXTRA)
    pick = (lanes_of(place) % seqs == rows_of(place)) & (lanes_of(place) < seqs * PARTS)
    raw = lax.dot_general(
        pick.astype(BF16), got_ref[:, lanes:], (((1,), (1,)), ((), ())), preferred_element_type=F32
    )
    place = (cols, cols)
    mean = (rows_of(place) // HEAD_DIM == lanes_of(place) // HEAD_DIM).astype(F32) / HEAD_DIM
    center = raw - jnp.dot(raw, mean, precision=EXACT)
    spread = jnp.dot(center * center, mean, precision=EXACT)
    normed = center * lax.rsqrt(spread + 1e-06) * gain_ref[...]
    read_ref[...] = normed[:seqs].astype(BF16)


def in_vmem(kernel, shapes, *operands):
    space = pl.BlockSpec(memory_space=pltpu.VMEM)
    many = isinstance(shapes, list)
    return pl.pallas_call(
        kernel,
        out_shape=shapes,
        in_specs=[space] * len(operands),
        out_specs=[space] * len(shapes) if many else space,
        compiler_params=pltpu.CompilerParams(vmem_limit_bytes=16 * 2**20),
    )(*operands)


def shards(
    tokens,
    key_weight,
    value_weight,
    log_decay,
    new_query,
    new_key,
    new_value,
    step_decay,
    norm_gain,
):
    seqs, span, width = tokens.shape
    heads = key_weight.shape[1] // HEAD_DIM
    cols = heads * HEAD_DIM
    lanes = seqs * HEAD_DIM
    half = HEAD_DIM // 2
    devices, mine = (lax.axis_size("sp"), lax.axis_index("sp"))
    rows = cols // devices

    positions = (mine * span + jnp.arange(span, dtype=jnp.int32)).astype(F32)
    inverse = 10000.0 ** (-jnp.arange(half, dtype=F32) * (2.0 / HEAD_DIM))
    angles = positions[:, None] * inverse
    cosine = jnp.tile(jnp.cos(angles), (1, 2 * heads)) * HEAD_DIM ** (-0.5)
    sine = jnp.sin(angles) * HEAD_DIM ** (-0.5)
    sine = jnp.tile(jnp.concatenate([-sine, sine], axis=1), (1, heads))
    totals = jnp.sum(log_decay, axis=-1)
    weight = jnp.exp(totals[:, :, None] - jnp.cumsum(log_decay, axis=-1))
    weight = jnp.transpose(weight, (1, 2, 0)).reshape(seqs * span, heads)
    carried = jnp.stack(in_three(totals), axis=-1).reshape(heads, 1, 1, seqs * PARTS)
    carried = jnp.broadcast_to(carried, (heads, devices // heads, 1, seqs * PARTS))
    carried = carried.reshape(devices, 1, seqs * PARTS)
    carried = jnp.pad(carried, ((0, 0), (0, rows - 1), (0, EXTRA - seqs * PARTS)))
    carried = carried.reshape(cols, EXTRA)

    end_pos = jnp.full((seqs, heads), float(span * devices), F32)
    query = rotate_half(new_query.astype(F32).reshape(seqs, heads, HEAD_DIM), end_pos)
    key_new = rotate_half(
        new_key.astype(F32).reshape(seqs, heads, HEAD_DIM), end_pos
    ) * HEAD_DIM ** (-0.5)
    decay_lanes = jnp.repeat(jnp.exp(step_decay), HEAD_DIM, axis=1)
    by_head = [jnp.transpose(x, (1, 0, 2)).reshape(heads, lanes) for x in (key_new, query)]
    lines = jnp.stack([decay_lanes, *by_head], axis=1)
    lines = lax.dynamic_index_in_dim(lines, mine // (devices // heads), 0, keepdims=False)
    value_cols = jnp.repeat(new_value.astype(F32).T, HEAD_DIM, axis=1)
    value_rows = lax.dynamic_slice_in_dim(value_cols, mine * rows, rows, 0)
    ready = lax.optimization_barrier((cosine, sine, weight, carried))
    cosine, sine, weight, carried = ready

    depth = key_weight.shape[0]
    own, spread = pl.pallas_call(
        spread_kernel,
        out_shape=[
            jax.ShapeDtypeStruct((depth, 2 * cols), BF16),
            jax.ShapeDtypeStruct((Y, depth, 2 * cols), BF16),
        ],
        in_specs=[pl.BlockSpec(memory_space=pl.ANY)] * 2,
        out_specs=[pl.BlockSpec(memory_space=pltpu.VMEM)] * 2,
        scratch_shapes=[pltpu.SemaphoreType.DMA((2 * (Y + 1),))],
    )(key_weight, value_weight)
    sums = projected(tokens.reshape(seqs * span, width), own, spread)
    whole = jax.ShapeDtypeStruct((cols, lanes + EXTRA), BF16)

    def exchanged(x):
        cut = x.reshape(devices, rows, lanes + EXTRA)
        return lax.all_to_all(cut, "sp", 0, 0, tiled=True).reshape(x.shape)

    sent = in_vmem(
        functools.partial(share_kernel, seqs), whole, sums, cosine, sine, weight, carried
    )
    finished = in_vmem(
        functools.partial(owner_kernel, devices, seqs), whole, exchanged(sent), lines, value_rows
    )
    gathered = exchanged(finished)
    gain = jnp.broadcast_to(norm_gain[None], (8, cols))
    state, first_read = in_vmem(
        functools.partial(read_kernel, seqs),
        [jax.ShapeDtypeStruct((cols, lanes), F32), jax.ShapeDtypeStruct((seqs, cols), BF16)],
        gathered,
        gain,
    )
    state_cache = jnp.transpose(state.reshape(heads, HEAD_DIM, lanes), (2, 0, 1))
    return (state_cache, first_read)


def solution(mesh):
    placed = (
        P("gr", "sp", None),
        P("sp", "tp"),
        P("sp", "tp"),
        P("tp", "gr", "sp"),
        P("gr", "tp"),
        P("gr", "tp"),
        P("gr", "tp"),
        P("tp", "gr"),
        P("tp"),
    )
    return jax.shard_map(
        shards,
        mesh=mesh,
        in_specs=placed,
        out_specs=(P("gr", "tp", None), P("gr", "tp")),
        check_vma=False,
    )
```

```python
import functools

import jax
import jax.numpy as jnp
from jax import lax
from jax.experimental import pallas as pl
from jax.experimental.pallas import tpu as pltpu
from jax.sharding import PartitionSpec as P

HEAD_DIM = 64
Y = 4
PARTS = 3
EXTRA = 128
EXACT = lax.Precision.HIGHEST
F32, BF16 = (jnp.float32, jnp.bfloat16)


def rotate_half(values, positions):
    half = values.shape[-1] // 2
    inverse = 10000.0 ** (-jnp.arange(half, dtype=jnp.float32) * (2.0 / values.shape[-1]))
    angles = positions[..., None] * inverse
    cosine = jnp.cos(angles)
    sine = jnp.sin(angles)
    first, second = (values[..., :half], values[..., half:])
    return jnp.concatenate(
        [first * cosine - second * sine, second * cosine + first * sine], axis=-1
    )


def moved_along_z(x, by):
    ring = lax.axis_size("gr") * lax.axis_size("sp") // Y
    pairs = [(z * Y + y, (z + by) % ring * Y + y) for z in range(ring) for y in range(Y)]
    return lax.ppermute(x, ("gr", "sp"), pairs)


def from_opposite_plane(x):
    ring = lax.axis_size("gr") * lax.axis_size("sp") // Y
    wide = lax.axis_size("tp")
    far = lax.axis_size("sp") // Y // 2
    pairs = []
    for z in range(ring):
        for y in range(Y):
            for t in range(wide):
                to = (z + (far if t % 2 else -far)) % ring
                pairs.append(((z * Y + y) * wide + t, (to * Y + y) * wide + t))
    return lax.ppermute(x, ("gr", "sp", "tp"), pairs)


def moved_along_y(x, by):
    planes = lax.axis_size("sp") // Y
    pairs = [(z * Y + y, z * Y + (y + by) % Y) for z in range(planes) for y in range(Y)]
    return lax.ppermute(x, "sp", pairs)


def exchanged_along_y(spread):
    groups = [[z * Y + y for y in range(Y)] for z in range(lax.axis_size("sp") // Y)]
    got = lax.all_to_all(spread, "sp", 0, 0, tiled=True, axis_index_groups=groups)
    return got.reshape(Y * got.shape[1], got.shape[2])


def projected(token_rows, own, spread):
    planes = lax.axis_size("sp") // Y
    far = planes // 2
    mine = lax.axis_index("sp").astype(jnp.uint32) // Y
    block = exchanged_along_y(spread)
    opposite = from_opposite_plane(own)
    depth = block.shape[0]
    row = lax.axis_index("sp").astype(jnp.uint32) % Y

    def part(weights, off, start=0):
        first = (mine + (off + planes)) % planes * depth + start
        cols = lax.dynamic_slice_in_dim(token_rows, first, weights.shape[0], 1)
        return jnp.dot(cols, weights, preferred_element_type=F32)

    def far_part(weights, by):
        return part(weights, far, (row + (Y - by)) % Y * own.shape[0])

    total = part(block, 0)
    up = down = block
    for hop in range(1, far):
        down = moved_along_z(down, -1)
        up = moved_along_z(up, 1)
        beside = moved_along_y(opposite, hop)
        if hop == 1:
            total += far_part(opposite, 0)
        total += far_part(beside, hop) + part(up, -hop) + part(down, hop)
    return total


def in_three(x):
    parts, rest = ([], x)
    for _ in range(PARTS):
        piece = lax.reduce_precision(rest, 8, 7)
        parts.append(piece.astype(jnp.bfloat16))
        rest = rest - piece
    return parts


def lanes_of(shape):
    return lax.broadcasted_iota(jnp.int32, shape, 1)


def rows_of(shape):
    return lax.broadcasted_iota(jnp.int32, shape, 0)


def spread_kernel(key_ref, value_ref, own_ref, spread_ref, sems):
    cols = key_ref.shape[1]
    copies = []
    for ref, cut in ((key_ref, pl.ds(0, cols)), (value_ref, pl.ds(cols, cols))):
        for to in (own_ref.at[:, cut], *(spread_ref.at[y, :, cut] for y in range(Y))):
            copies.append(pltpu.make_async_copy(ref, to, sems.at[len(copies)]))
    for copy in copies:
        copy.start()
    for copy in copies:
        copy.wait()


def share_kernel(seqs, sums_ref, cosine_ref, sine_ref, weight_ref, carried_ref, out_ref):
    cols = out_ref.shape[0]
    heads = cols // HEAD_DIM
    span = sums_ref.shape[0] // seqs
    half = HEAD_DIM // 2
    low = lanes_of((span, cols)) % HEAD_DIM < half
    spread = (rows_of((heads, cols)) == lanes_of((heads, cols)) // HEAD_DIM).astype(F32)
    blocks = [[] for _ in range(heads)]
    for seq in range(seqs):
        here = pl.ds(seq * span, span)
        keys = sums_ref[here, :cols].astype(BF16).astype(F32)
        values = sums_ref[here, cols:].astype(BF16)
        other = jnp.where(low, pltpu.roll(keys, cols - half, 1), pltpu.roll(keys, half, 1))
        turned = keys * cosine_ref[...] + other * sine_ref[...]
        faded = turned * jnp.dot(weight_ref[here, :], spread, precision=EXACT)
        high = faded.astype(BF16)
        rest = (faded - high.astype(F32)).astype(BF16)
        product = sum(
            lax.dot_general(
                values, part, (((0,), (0,)), ((), ())), preferred_element_type=F32
            )
            for part in (high, rest)
        )
        for head in range(heads):
            cut = slice(head * HEAD_DIM, (head + 1) * HEAD_DIM)
            blocks[head].append(product[cut, cut])
    for head in range(heads):
        cut = pl.ds(head * HEAD_DIM, HEAD_DIM)
        out_ref[cut, : seqs * HEAD_DIM] = jnp.concatenate(blocks[head], axis=1).astype(BF16)
    out_ref[:, seqs * HEAD_DIM :] = carried_ref[...]


def owner_kernel(devices, seqs, got_ref, lines_ref, values_ref, out_ref):
    total, lanes = (got_ref.shape[0], seqs * HEAD_DIM)
    rows = total // devices
    later = (lanes_of((devices, total)) // rows > rows_of((devices, total))) & (
        lanes_of((devices, total)) % rows == 0
    )
    sums = jnp.dot(later.astype(BF16), got_ref[:, lanes:], preferred_element_type=F32)
    place = (EXTRA, lanes)
    wide = (rows_of(place) // PARTS == lanes_of(place) // HEAD_DIM).astype(F32)
    fade = jnp.exp(jnp.dot(sums, wide, precision=EXACT))
    shares = got_ref[:, :lanes].astype(F32)
    owned = shares[:rows] * fade[0:1]
    for device in range(1, devices):
        owned += shares[device * rows : (device + 1) * rows] * fade[device : device + 1]
    finished = lines_ref[0:1] * owned + lines_ref[1:2] * values_ref[...]
    place = (lanes, EXTRA)
    fold = rows_of(place) // HEAD_DIM == lanes_of(place) % seqs
    read = jnp.dot(finished * lines_ref[2:3], fold.astype(F32), precision=EXACT)
    piece = lanes_of(read.shape) // seqs
    rest, packed = (read, jnp.zeros_like(read))
    for part in range(PARTS):
        rounded = rest.astype(BF16).astype(F32)
        packed = jnp.where(piece == part, rounded, packed)
        rest = rest - rounded
    line = jnp.concatenate([finished, packed], axis=1)
    out_ref[...] = jnp.concatenate([line] * devices, axis=0).astype(BF16)


def read_kernel(seqs, got_ref, gain_ref, state_ref, read_ref):
    cols, lanes = (got_ref.shape[0], seqs * HEAD_DIM)
    state_ref[...] = got_ref[:, :lanes].astype(F32)
    place = (8, EXTRA)
    pick = (lanes_of(place) % seqs == rows_of(place)) & (lanes_of(place) < seqs * PARTS)
    raw = lax.dot_general(
        pick.astype(BF16), got_ref[:, lanes:], (((1,), (1,)), ((), ())), preferred_element_type=F32
    )
    place = (cols, cols)
    mean = (rows_of(place) // HEAD_DIM == lanes_of(place) // HEAD_DIM).astype(F32) / HEAD_DIM
    center = raw - jnp.dot(raw, mean, precision=EXACT)
    spread = jnp.dot(center * center, mean, precision=EXACT)
    normed = center * lax.rsqrt(spread + 1e-06) * gain_ref[...]
    read_ref[...] = normed[:seqs].astype(BF16)


def in_vmem(kernel, shapes, *operands):
    space = pl.BlockSpec(memory_space=pltpu.VMEM)
    many = isinstance(shapes, list)
    return pl.pallas_call(
        kernel,
        out_shape=shapes,
        in_specs=[space] * len(operands),
        out_specs=[space] * len(shapes) if many else space,
        compiler_params=pltpu.CompilerParams(vmem_limit_bytes=16 * 2**20),
    )(*operands)


def shards(
    tokens,
    key_weight,
    value_weight,
    log_decay,
    new_query,
    new_key,
    new_value,
    step_decay,
    norm_gain,
):
    seqs, span, width = tokens.shape
    heads = key_weight.shape[1] // HEAD_DIM
    cols = heads * HEAD_DIM
    lanes = seqs * HEAD_DIM
    half = HEAD_DIM // 2
    devices, mine = (lax.axis_size("sp"), lax.axis_index("sp"))
    rows = cols // devices

    positions = (mine * span + jnp.arange(span, dtype=jnp.int32)).astype(F32)
    inverse = 10000.0 ** (-jnp.arange(half, dtype=F32) * (2.0 / HEAD_DIM))
    angles = positions[:, None] * inverse
    cosine = jnp.tile(jnp.cos(angles), (1, 2 * heads)) * HEAD_DIM ** (-0.5)
    sine = jnp.sin(angles) * HEAD_DIM ** (-0.5)
    sine = jnp.tile(jnp.concatenate([-sine, sine], axis=1), (1, heads))
    totals = jnp.sum(log_decay, axis=-1)
    weight = jnp.exp(totals[:, :, None] - jnp.cumsum(log_decay, axis=-1))
    weight = jnp.transpose(weight, (1, 2, 0)).reshape(seqs * span, heads)
    carried = jnp.stack(in_three(totals), axis=-1).reshape(heads, 1, 1, seqs * PARTS)
    carried = jnp.broadcast_to(carried, (heads, devices // heads, 1, seqs * PARTS))
    carried = carried.reshape(devices, 1, seqs * PARTS)
    carried = jnp.pad(carried, ((0, 0), (0, rows - 1), (0, EXTRA - seqs * PARTS)))
    carried = carried.reshape(cols, EXTRA)

    end_pos = jnp.full((seqs, heads), float(span * devices), F32)
    query = rotate_half(new_query.astype(F32).reshape(seqs, heads, HEAD_DIM), end_pos)
    key_new = rotate_half(
        new_key.astype(F32).reshape(seqs, heads, HEAD_DIM), end_pos
    ) * HEAD_DIM ** (-0.5)
    decay_lanes = jnp.repeat(jnp.exp(step_decay), HEAD_DIM, axis=1)
    by_head = [jnp.transpose(x, (1, 0, 2)).reshape(heads, lanes) for x in (key_new, query)]
    lines = jnp.stack([decay_lanes, *by_head], axis=1)
    lines = lax.dynamic_index_in_dim(lines, mine // (devices // heads), 0, keepdims=False)
    value_cols = jnp.repeat(new_value.astype(F32).T, HEAD_DIM, axis=1)
    value_rows = lax.dynamic_slice_in_dim(value_cols, mine * rows, rows, 0)
    ready = lax.optimization_barrier((cosine, sine, weight, carried, lines, value_rows))
    cosine, sine, weight, carried, lines, value_rows = ready

    depth = key_weight.shape[0]
    own, spread = pl.pallas_call(
        spread_kernel,
        out_shape=[
            jax.ShapeDtypeStruct((depth, 2 * cols), BF16),
            jax.ShapeDtypeStruct((Y, depth, 2 * cols), BF16),
        ],
        in_specs=[pl.BlockSpec(memory_space=pl.ANY)] * 2,
        out_specs=[pl.BlockSpec(memory_space=pltpu.VMEM)] * 2,
        scratch_shapes=[pltpu.SemaphoreType.DMA((2 * (Y + 1),))],
    )(key_weight, value_weight)
    sums = projected(tokens.reshape(seqs * span, width), own, spread)
    whole = jax.ShapeDtypeStruct((cols, lanes + EXTRA), BF16)

    def exchanged(x):
        cut = x.reshape(devices, rows, lanes + EXTRA)
        return lax.all_to_all(cut, "sp", 0, 0, tiled=True).reshape(x.shape)

    sent = in_vmem(
        functools.partial(share_kernel, seqs), whole, sums, cosine, sine, weight, carried
    )
    finished = in_vmem(
        functools.partial(owner_kernel, devices, seqs), whole, exchanged(sent), lines, value_rows
    )
    state, first_read = in_vmem(
        functools.partial(read_kernel, seqs),
        [jax.ShapeDtypeStruct((cols, lanes), F32), jax.ShapeDtypeStruct((seqs, cols), BF16)],
        exchanged(finished),
        norm_gain.reshape(1, cols),
    )
    state_cache = jnp.transpose(state.reshape(heads, HEAD_DIM, lanes), (2, 0, 1))
    return (state_cache, first_read)


def solution(mesh):
    placed = (
        P("gr", "sp", None),
        P("sp", "tp"),
        P("sp", "tp"),
        P("tp", "gr", "sp"),
        P("gr", "tp"),
        P("gr", "tp"),
        P("gr", "tp"),
        P("tp", "gr"),
        P("tp"),
    )
    return jax.shard_map(
        shards,
        mesh=mesh,
        in_specs=placed,
        out_specs=(P("gr", "tp", None), P("gr", "tp")),
        check_vma=False,
    )
```

```python
import functools

import jax
import jax.numpy as jnp
from jax import lax
from jax.experimental import pallas as pl
from jax.experimental.pallas import tpu as pltpu
from jax.sharding import PartitionSpec as P

HEAD_DIM = 64
Y = 4
PARTS = 3
EXTRA = 128
EXACT = lax.Precision.HIGHEST
F32, BF16 = (jnp.float32, jnp.bfloat16)


def moved_along_z(x, by):
    ring = lax.axis_size("gr") * lax.axis_size("sp") // Y
    pairs = [(z * Y + y, (z + by) % ring * Y + y) for z in range(ring) for y in range(Y)]
    return lax.ppermute(x, ("gr", "sp"), pairs)


def from_opposite_plane(x):
    ring = lax.axis_size("gr") * lax.axis_size("sp") // Y
    wide = lax.axis_size("tp")
    far = lax.axis_size("sp") // Y // 2
    pairs = []
    for z in range(ring):
        for y in range(Y):
            for t in range(wide):
                to = (z + (far if t % 2 else -far)) % ring
                pairs.append(((z * Y + y) * wide + t, (to * Y + y) * wide + t))
    return lax.ppermute(x, ("gr", "sp", "tp"), pairs)


def moved_along_y(x, by):
    planes = lax.axis_size("sp") // Y
    pairs = [(z * Y + y, z * Y + (y + by) % Y) for z in range(planes) for y in range(Y)]
    return lax.ppermute(x, "sp", pairs)


def exchanged_along_y(spread):
    groups = [[z * Y + y for y in range(Y)] for z in range(lax.axis_size("sp") // Y)]
    got = lax.all_to_all(spread, "sp", 0, 0, tiled=True, axis_index_groups=groups)
    return got.reshape(Y * got.shape[1], got.shape[2])


def projected(token_rows, own, spread):
    planes = lax.axis_size("sp") // Y
    far = planes // 2
    mine = lax.axis_index("sp").astype(jnp.uint32) // Y
    block = exchanged_along_y(spread)
    opposite = from_opposite_plane(own)
    depth = block.shape[0]
    row = lax.axis_index("sp").astype(jnp.uint32) % Y

    def part(weights, off, start=0):
        first = (mine + (off + planes)) % planes * depth + start
        cols = lax.dynamic_slice_in_dim(token_rows, first, weights.shape[0], 1)
        return jnp.dot(cols, weights, preferred_element_type=F32)

    def far_part(weights, by):
        return part(weights, far, (row + (Y - by)) % Y * own.shape[0])

    total = part(block, 0)
    up = down = block
    for hop in range(1, far):
        down = moved_along_z(down, -1)
        up = moved_along_z(up, 1)
        beside = moved_along_y(opposite, hop)
        if hop == 1:
            total += far_part(opposite, 0)
        total += far_part(beside, hop) + part(up, -hop) + part(down, hop)
    return total


def in_three(x):
    parts, rest = ([], x)
    for _ in range(PARTS):
        piece = lax.reduce_precision(rest, 8, 7)
        parts.append(piece.astype(jnp.bfloat16))
        rest = rest - piece
    return parts


def lanes_of(shape):
    return lax.broadcasted_iota(jnp.int32, shape, 1)


def rows_of(shape):
    return lax.broadcasted_iota(jnp.int32, shape, 0)


def spread_kernel(key_ref, value_ref, own_ref, spread_ref, sems):
    cols = key_ref.shape[1]
    copies = []
    for ref, cut in ((key_ref, pl.ds(0, cols)), (value_ref, pl.ds(cols, cols))):
        for to in (own_ref.at[:, cut], *(spread_ref.at[y, :, cut] for y in range(Y))):
            copies.append(pltpu.make_async_copy(ref, to, sems.at[len(copies)]))
    for copy in copies:
        copy.start()
    for copy in copies:
        copy.wait()


def share_kernel(seqs, sums_ref, cosine_ref, sine_ref, weight_ref, carried_ref, out_ref):
    cols = out_ref.shape[0]
    heads = cols // HEAD_DIM
    span = sums_ref.shape[0] // seqs
    half = HEAD_DIM // 2
    low = lanes_of((span, cols)) % HEAD_DIM < half
    spread = (rows_of((heads, cols)) == lanes_of((heads, cols)) // HEAD_DIM).astype(F32)
    blocks = [[] for _ in range(heads)]
    for seq in range(seqs):
        here = pl.ds(seq * span, span)
        keys = sums_ref[here, :cols].astype(BF16).astype(F32)
        values = sums_ref[here, cols:].astype(BF16)
        other = jnp.where(low, pltpu.roll(keys, cols - half, 1), pltpu.roll(keys, half, 1))
        turned = keys * cosine_ref[...] + other * sine_ref[...]
        faded = turned * jnp.dot(weight_ref[here, :], spread, precision=EXACT)
        high = faded.astype(BF16)
        rest = (faded - high.astype(F32)).astype(BF16)
        product = sum(
            lax.dot_general(
                values, part, (((0,), (0,)), ((), ())), preferred_element_type=F32
            )
            for part in (high, rest)
        )
        for head in range(heads):
            cut = slice(head * HEAD_DIM, (head + 1) * HEAD_DIM)
            blocks[head].append(product[cut, cut])
    for head in range(heads):
        cut = pl.ds(head * HEAD_DIM, HEAD_DIM)
        out_ref[cut, : seqs * HEAD_DIM] = jnp.concatenate(blocks[head], axis=1).astype(BF16)
    out_ref[:, seqs * HEAD_DIM :] = carried_ref[...]


def lines_kernel(
    place_ref, cosine_ref, sine_ref, query_ref, key_ref, value_ref, decay_ref, lines_ref, values_ref
):
    seqs, cols = query_ref.shape
    heads, lanes = (cols // HEAD_DIM, seqs * HEAD_DIM)
    rows, half = (values_ref.shape[0], HEAD_DIM // 2)
    mine = place_ref[0]
    head = mine * rows // HEAD_DIM
    low = lanes_of((seqs, cols)) % HEAD_DIM < half
    place = (cols, lanes)
    pick = (rows_of(place) // HEAD_DIM == head) & (
        rows_of(place) % HEAD_DIM == lanes_of(place) % HEAD_DIM
    )
    own = rows_of((seqs, lanes)) == lanes_of((seqs, lanes)) // HEAD_DIM

    def line(ref):
        u = ref[...].astype(F32)
        other = jnp.where(low, pltpu.roll(u, cols - half, 1), pltpu.roll(u, half, 1))
        turned = u * cosine_ref[...] + other * sine_ref[...]
        picked = jnp.dot(turned, pick.astype(F32), precision=EXACT)
        return jnp.sum(jnp.where(own, picked, 0.0), axis=0, keepdims=True)

    decay = jnp.dot(jnp.exp(decay_ref[...]), own.astype(F32), precision=EXACT)
    here = rows_of((heads, lanes)) == head
    lines_ref[0:1] = jnp.sum(jnp.where(here, decay, 0.0), axis=0, keepdims=True)
    lines_ref[1:2] = line(key_ref) * HEAD_DIM ** (-0.5)
    lines_ref[2:3] = line(query_ref)
    spot = lanes_of((rows, cols)) == mine * rows + rows_of((rows, cols))
    values = lax.dot_general(
        spot.astype(BF16), value_ref[...], (((1,), (1,)), ((), ())), preferred_element_type=F32
    )
    values_ref[...] = jnp.dot(values, own.astype(F32), precision=EXACT)


def owner_kernel(devices, seqs, got_ref, lines_ref, values_ref, out_ref):
    total, lanes = (got_ref.shape[0], seqs * HEAD_DIM)
    rows = total // devices
    later = (lanes_of((devices, total)) // rows > rows_of((devices, total))) & (
        lanes_of((devices, total)) % rows == 0
    )
    sums = jnp.dot(later.astype(BF16), got_ref[:, lanes:], preferred_element_type=F32)
    place = (EXTRA, lanes)
    wide = (rows_of(place) // PARTS == lanes_of(place) // HEAD_DIM).astype(F32)
    fade = jnp.exp(jnp.dot(sums, wide, precision=EXACT))
    shares = got_ref[:, :lanes].astype(F32)
    owned = shares[:rows] * fade[0:1]
    for device in range(1, devices):
        owned += shares[device * rows : (device + 1) * rows] * fade[device : device + 1]
    finished = lines_ref[0:1] * owned + lines_ref[1:2] * values_ref[...]
    place = (lanes, EXTRA)
    fold = rows_of(place) // HEAD_DIM == lanes_of(place) % seqs
    read = jnp.dot(finished * lines_ref[2:3], fold.astype(F32), precision=EXACT)
    piece = lanes_of(read.shape) // seqs
    rest, packed = (read, jnp.zeros_like(read))
    for part in range(PARTS):
        rounded = rest.astype(BF16).astype(F32)
        packed = jnp.where(piece == part, rounded, packed)
        rest = rest - rounded
    line = jnp.concatenate([finished, packed], axis=1)
    out_ref[...] = jnp.concatenate([line] * devices, axis=0).astype(BF16)


def read_kernel(seqs, got_ref, gain_ref, state_ref, read_ref):
    cols, lanes = (got_ref.shape[0], seqs * HEAD_DIM)
    state_ref[...] = got_ref[:, :lanes].astype(F32)
    place = (8, EXTRA)
    pick = (lanes_of(place) % seqs == rows_of(place)) & (lanes_of(place) < seqs * PARTS)
    raw = lax.dot_general(
        pick.astype(BF16), got_ref[:, lanes:], (((1,), (1,)), ((), ())), preferred_element_type=F32
    )
    place = (cols, cols)
    mean = (rows_of(place) // HEAD_DIM == lanes_of(place) // HEAD_DIM).astype(F32) / HEAD_DIM
    center = raw - jnp.dot(raw, mean, precision=EXACT)
    spread = jnp.dot(center * center, mean, precision=EXACT)
    normed = center * lax.rsqrt(spread + 1e-06) * gain_ref[...]
    read_ref[...] = normed[:seqs].astype(BF16)


def in_vmem(kernel, shapes, *operands):
    space = pl.BlockSpec(memory_space=pltpu.VMEM)
    many = isinstance(shapes, list)
    return pl.pallas_call(
        kernel,
        out_shape=shapes,
        in_specs=[space] * len(operands),
        out_specs=[space] * len(shapes) if many else space,
        compiler_params=pltpu.CompilerParams(vmem_limit_bytes=16 * 2**20),
    )(*operands)


def shards(
    tokens,
    key_weight,
    value_weight,
    log_decay,
    new_query,
    new_key,
    new_value,
    step_decay,
    norm_gain,
):
    seqs, span, width = tokens.shape
    heads = key_weight.shape[1] // HEAD_DIM
    cols = heads * HEAD_DIM
    lanes = seqs * HEAD_DIM
    half = HEAD_DIM // 2
    devices, mine = (lax.axis_size("sp"), lax.axis_index("sp"))
    rows = cols // devices

    positions = (mine * span + jnp.arange(span, dtype=jnp.int32)).astype(F32)
    inverse = 10000.0 ** (-jnp.arange(half, dtype=F32) * (2.0 / HEAD_DIM))
    angles = positions[:, None] * inverse
    cosine = jnp.tile(jnp.cos(angles), (1, 2 * heads)) * HEAD_DIM ** (-0.5)
    sine = jnp.sin(angles) * HEAD_DIM ** (-0.5)
    sine = jnp.tile(jnp.concatenate([-sine, sine], axis=1), (1, heads))
    totals = jnp.sum(log_decay, axis=-1)
    weight = jnp.exp(totals[:, :, None] - jnp.cumsum(log_decay, axis=-1))
    weight = jnp.transpose(weight, (1, 2, 0)).reshape(seqs * span, heads)
    carried = jnp.stack(in_three(totals), axis=-1).reshape(heads, 1, 1, seqs * PARTS)
    carried = jnp.broadcast_to(carried, (heads, devices // heads, 1, seqs * PARTS))
    carried = carried.reshape(devices, 1, seqs * PARTS)
    carried = jnp.pad(carried, ((0, 0), (0, rows - 1), (0, EXTRA - seqs * PARTS)))
    carried = carried.reshape(cols, EXTRA)

    last = float(span * devices) * inverse
    last_cosine = jnp.tile(jnp.cos(last), 2 * heads)[None]
    last_sine = jnp.sin(last)
    last_sine = jnp.tile(jnp.concatenate([-last_sine, last_sine]), heads)[None]
    ready = (cosine, sine, weight, carried, last_cosine, last_sine)
    cosine, sine, weight, carried, last_cosine, last_sine = lax.optimization_barrier(ready)

    depth = key_weight.shape[0]
    own, spread = pl.pallas_call(
        spread_kernel,
        out_shape=[
            jax.ShapeDtypeStruct((depth, 2 * cols), BF16),
            jax.ShapeDtypeStruct((Y, depth, 2 * cols), BF16),
        ],
        in_specs=[pl.BlockSpec(memory_space=pl.ANY)] * 2,
        out_specs=[pl.BlockSpec(memory_space=pltpu.VMEM)] * 2,
        scratch_shapes=[pltpu.SemaphoreType.DMA((2 * (Y + 1),))],
    )(key_weight, value_weight)
    sums = projected(tokens.reshape(seqs * span, width), own, spread)
    place = pl.BlockSpec(memory_space=pltpu.SMEM)
    space = pl.BlockSpec(memory_space=pltpu.VMEM)
    lines, value_rows = pl.pallas_call(
        lines_kernel,
        out_shape=[jax.ShapeDtypeStruct((3, lanes), F32), jax.ShapeDtypeStruct((rows, lanes), F32)],
        in_specs=[place] + [space] * 6,
        out_specs=[space] * 2,
        compiler_params=pltpu.CompilerParams(vmem_limit_bytes=2 * 2**20),
    )(
        mine[None],
        last_cosine,
        last_sine,
        new_query,
        new_key,
        new_value,
        step_decay,
    )
    whole = jax.ShapeDtypeStruct((cols, lanes + EXTRA), BF16)

    def exchanged(x):
        cut = x.reshape(devices, rows, lanes + EXTRA)
        return lax.all_to_all(cut, "sp", 0, 0, tiled=True).reshape(x.shape)

    sent = in_vmem(
        functools.partial(share_kernel, seqs), whole, sums, cosine, sine, weight, carried
    )
    finished = in_vmem(
        functools.partial(owner_kernel, devices, seqs), whole, exchanged(sent), lines, value_rows
    )
    state, first_read = in_vmem(
        functools.partial(read_kernel, seqs),
        [jax.ShapeDtypeStruct((cols, lanes), F32), jax.ShapeDtypeStruct((seqs, cols), BF16)],
        exchanged(finished),
        norm_gain.reshape(1, cols),
    )
    state_cache = jnp.transpose(state.reshape(heads, HEAD_DIM, lanes), (2, 0, 1))
    return (state_cache, first_read)


def solution(mesh):
    placed = (
        P("gr", "sp", None),
        P("sp", "tp"),
        P("sp", "tp"),
        P("tp", "gr", "sp"),
        P("gr", "tp"),
        P("gr", "tp"),
        P("gr", "tp"),
        P("tp", "gr"),
        P("tp"),
    )
    return jax.shard_map(
        shards,
        mesh=mesh,
        in_specs=placed,
        out_specs=(P("gr", "tp", None), P("gr", "tp")),
        check_vma=False,
    )
```

```python
import functools

import jax
import jax.numpy as jnp
from jax import lax
from jax.experimental import pallas as pl
from jax.experimental.pallas import tpu as pltpu
from jax.sharding import PartitionSpec as P

HEAD_DIM = 64
Y = 4
PARTS = 3
EXTRA = 128
EXACT = lax.Precision.HIGHEST
F32, BF16 = (jnp.float32, jnp.bfloat16)


def moved_along_z(x, by):
    ring = lax.axis_size("gr") * lax.axis_size("sp") // Y
    pairs = [(z * Y + y, (z + by) % ring * Y + y) for z in range(ring) for y in range(Y)]
    return lax.ppermute(x, ("gr", "sp"), pairs)


def from_opposite_plane(x):
    ring = lax.axis_size("gr") * lax.axis_size("sp") // Y
    wide = lax.axis_size("tp")
    far = lax.axis_size("sp") // Y // 2
    pairs = []
    for z in range(ring):
        for y in range(Y):
            for t in range(wide):
                to = (z + (far if t % 2 else -far)) % ring
                pairs.append(((z * Y + y) * wide + t, (to * Y + y) * wide + t))
    return lax.ppermute(x, ("gr", "sp", "tp"), pairs)


def moved_along_y(x, by):
    planes = lax.axis_size("sp") // Y
    pairs = [(z * Y + y, z * Y + (y + by) % Y) for z in range(planes) for y in range(Y)]
    return lax.ppermute(x, "sp", pairs)


def exchanged_along_y(spread):
    groups = [[z * Y + y for y in range(Y)] for z in range(lax.axis_size("sp") // Y)]
    got = lax.all_to_all(spread, "sp", 0, 0, tiled=True, axis_index_groups=groups)
    return got.reshape(Y * got.shape[1], got.shape[2])


def projected(token_rows, own, spread):
    planes = lax.axis_size("sp") // Y
    far = planes // 2
    mine = lax.axis_index("sp").astype(jnp.uint32) // Y
    block = exchanged_along_y(spread)
    opposite = from_opposite_plane(own)
    depth = block.shape[0]
    row = lax.axis_index("sp").astype(jnp.uint32) % Y

    def part(weights, off, start=0):
        first = (mine + (off + planes)) % planes * depth + start
        cols = lax.dynamic_slice_in_dim(token_rows, first, weights.shape[0], 1)
        return jnp.dot(cols, weights, preferred_element_type=F32)

    def far_part(weights, by):
        return part(weights, far, (row + (Y - by)) % Y * own.shape[0])

    total = part(block, 0)
    up = down = block
    for hop in range(1, far):
        down = moved_along_z(down, -1)
        up = moved_along_z(up, 1)
        beside = moved_along_y(opposite, hop)
        if hop == 1:
            total += far_part(opposite, 0)
        total += far_part(beside, hop) + part(up, -hop) + part(down, hop)
    return total


def in_three(x):
    parts, rest = ([], x)
    for _ in range(PARTS):
        piece = lax.reduce_precision(rest, 8, 7)
        parts.append(piece.astype(jnp.bfloat16))
        rest = rest - piece
    return parts


def lanes_of(shape):
    return lax.broadcasted_iota(jnp.int32, shape, 1)


def rows_of(shape):
    return lax.broadcasted_iota(jnp.int32, shape, 0)


def spread_kernel(key_ref, value_ref, own_ref, spread_ref, in_sems, out_sems):
    cols = key_ref.shape[1]
    cuts = (pl.ds(0, cols), pl.ds(cols, cols))
    loads = [
        pltpu.make_async_copy(ref, own_ref.at[:, cut], in_sems.at[n])
        for n, (ref, cut) in enumerate(zip((key_ref, value_ref), cuts))
    ]
    for load in loads:
        load.start()
    copies = []
    for load, cut in zip(loads, cuts):
        load.wait()
        for y in range(Y):
            to = spread_ref.at[y, :, cut]
            copies.append(pltpu.make_async_copy(own_ref.at[:, cut], to, out_sems.at[len(copies)]))
            copies[-1].start()
    for copy in copies:
        copy.wait()


def share_kernel(seqs, sums_ref, cosine_ref, sine_ref, weight_ref, carried_ref, out_ref):
    cols = out_ref.shape[0]
    heads = cols // HEAD_DIM
    span = sums_ref.shape[0] // seqs
    half = HEAD_DIM // 2
    low = lanes_of((span, cols)) % HEAD_DIM < half
    spread = (rows_of((heads, cols)) == lanes_of((heads, cols)) // HEAD_DIM).astype(F32)
    blocks = [[] for _ in range(heads)]
    for seq in range(seqs):
        here = pl.ds(seq * span, span)
        keys = sums_ref[here, :cols].astype(BF16).astype(F32)
        values = sums_ref[here, cols:].astype(BF16)
        other = jnp.where(low, pltpu.roll(keys, cols - half, 1), pltpu.roll(keys, half, 1))
        turned = keys * cosine_ref[...] + other * sine_ref[...]
        faded = turned * jnp.dot(weight_ref[here, :], spread, precision=EXACT)
        high = faded.astype(BF16)
        rest = (faded - high.astype(F32)).astype(BF16)
        product = sum(
            lax.dot_general(
                values, part, (((0,), (0,)), ((), ())), preferred_element_type=F32
            )
            for part in (high, rest)
        )
        for head in range(heads):
            cut = slice(head * HEAD_DIM, (head + 1) * HEAD_DIM)
            blocks[head].append(product[cut, cut])
    for head in range(heads):
        cut = pl.ds(head * HEAD_DIM, HEAD_DIM)
        out_ref[cut, : seqs * HEAD_DIM] = jnp.concatenate(blocks[head], axis=1).astype(BF16)
    out_ref[:, seqs * HEAD_DIM :] = carried_ref[...]


def lines_kernel(
    place_ref, cosine_ref, sine_ref, query_ref, key_ref, value_ref, decay_ref, lines_ref, values_ref
):
    seqs, cols = query_ref.shape
    heads, lanes = (cols // HEAD_DIM, seqs * HEAD_DIM)
    rows, half = (values_ref.shape[0], HEAD_DIM // 2)
    mine = place_ref[0]
    head = mine * rows // HEAD_DIM
    low = lanes_of((seqs, cols)) % HEAD_DIM < half
    place = (cols, lanes)
    pick = (rows_of(place) // HEAD_DIM == head) & (
        rows_of(place) % HEAD_DIM == lanes_of(place) % HEAD_DIM
    )
    own = rows_of((seqs, lanes)) == lanes_of((seqs, lanes)) // HEAD_DIM

    def line(ref):
        u = ref[...].astype(F32)
        other = jnp.where(low, pltpu.roll(u, cols - half, 1), pltpu.roll(u, half, 1))
        turned = u * cosine_ref[...] + other * sine_ref[...]
        picked = jnp.dot(turned, pick.astype(F32), precision=EXACT)
        return jnp.sum(jnp.where(own, picked, 0.0), axis=0, keepdims=True)

    decay = jnp.dot(jnp.exp(decay_ref[...]), own.astype(F32), precision=EXACT)
    here = rows_of((heads, lanes)) == head
    lines_ref[0:1] = jnp.sum(jnp.where(here, decay, 0.0), axis=0, keepdims=True)
    lines_ref[1:2] = line(key_ref) * HEAD_DIM ** (-0.5)
    lines_ref[2:3] = line(query_ref)
    spot = lanes_of((rows, cols)) == mine * rows + rows_of((rows, cols))
    values = lax.dot_general(
        spot.astype(BF16), value_ref[...], (((1,), (1,)), ((), ())), preferred_element_type=F32
    )
    values_ref[...] = jnp.dot(values, own.astype(F32), precision=EXACT)


def owner_kernel(devices, seqs, got_ref, lines_ref, values_ref, out_ref):
    total, lanes = (got_ref.shape[0], seqs * HEAD_DIM)
    rows = total // devices
    later = (lanes_of((devices, total)) // rows > rows_of((devices, total))) & (
        lanes_of((devices, total)) % rows == 0
    )
    sums = jnp.dot(later.astype(BF16), got_ref[:, lanes:], preferred_element_type=F32)
    place = (EXTRA, lanes)
    wide = (rows_of(place) // PARTS == lanes_of(place) // HEAD_DIM).astype(F32)
    fade = jnp.exp(jnp.dot(sums, wide, precision=EXACT))
    shares = got_ref[:, :lanes].astype(F32)
    owned = shares[:rows] * fade[0:1]
    for device in range(1, devices):
        owned += shares[device * rows : (device + 1) * rows] * fade[device : device + 1]
    finished = lines_ref[0:1] * owned + lines_ref[1:2] * values_ref[...]
    place = (lanes, EXTRA)
    fold = rows_of(place) // HEAD_DIM == lanes_of(place) % seqs
    read = jnp.dot(finished * lines_ref[2:3], fold.astype(F32), precision=EXACT)
    piece = lanes_of(read.shape) // seqs
    rest, packed = (read, jnp.zeros_like(read))
    for part in range(PARTS):
        rounded = rest.astype(BF16).astype(F32)
        packed = jnp.where(piece == part, rounded, packed)
        rest = rest - rounded
    line = jnp.concatenate([finished, packed], axis=1)
    out_ref[...] = jnp.concatenate([line] * devices, axis=0).astype(BF16)


def read_kernel(seqs, got_ref, gain_ref, state_ref, read_ref):
    cols, lanes = (got_ref.shape[0], seqs * HEAD_DIM)
    state_ref[...] = got_ref[:, :lanes].astype(F32)
    place = (8, EXTRA)
    pick = (lanes_of(place) % seqs == rows_of(place)) & (lanes_of(place) < seqs * PARTS)
    raw = lax.dot_general(
        pick.astype(BF16), got_ref[:, lanes:], (((1,), (1,)), ((), ())), preferred_element_type=F32
    )
    place = (cols, cols)
    mean = (rows_of(place) // HEAD_DIM == lanes_of(place) // HEAD_DIM).astype(F32) / HEAD_DIM
    center = raw - jnp.dot(raw, mean, precision=EXACT)
    spread = jnp.dot(center * center, mean, precision=EXACT)
    normed = center * lax.rsqrt(spread + 1e-06) * gain_ref[...]
    read_ref[...] = normed[:seqs].astype(BF16)


def in_vmem(kernel, shapes, *operands):
    space = pl.BlockSpec(memory_space=pltpu.VMEM)
    many = isinstance(shapes, list)
    return pl.pallas_call(
        kernel,
        out_shape=shapes,
        in_specs=[space] * len(operands),
        out_specs=[space] * len(shapes) if many else space,
        compiler_params=pltpu.CompilerParams(vmem_limit_bytes=16 * 2**20),
    )(*operands)


def shards(
    tokens,
    key_weight,
    value_weight,
    log_decay,
    new_query,
    new_key,
    new_value,
    step_decay,
    norm_gain,
):
    seqs, span, width = tokens.shape
    heads = key_weight.shape[1] // HEAD_DIM
    cols = heads * HEAD_DIM
    lanes = seqs * HEAD_DIM
    half = HEAD_DIM // 2
    devices, mine = (lax.axis_size("sp"), lax.axis_index("sp"))
    rows = cols // devices

    positions = (mine * span + jnp.arange(span, dtype=jnp.int32)).astype(F32)
    inverse = 10000.0 ** (-jnp.arange(half, dtype=F32) * (2.0 / HEAD_DIM))
    angles = positions[:, None] * inverse
    cosine = jnp.tile(jnp.cos(angles), (1, 2 * heads)) * HEAD_DIM ** (-0.5)
    sine = jnp.sin(angles) * HEAD_DIM ** (-0.5)
    sine = jnp.tile(jnp.concatenate([-sine, sine], axis=1), (1, heads))
    totals = jnp.sum(log_decay, axis=-1)
    weight = jnp.exp(totals[:, :, None] - jnp.cumsum(log_decay, axis=-1))
    weight = jnp.transpose(weight, (1, 2, 0)).reshape(seqs * span, heads)
    carried = jnp.stack(in_three(totals), axis=-1).reshape(heads, 1, 1, seqs * PARTS)
    carried = jnp.broadcast_to(carried, (heads, devices // heads, 1, seqs * PARTS))
    carried = carried.reshape(devices, 1, seqs * PARTS)
    carried = jnp.pad(carried, ((0, 0), (0, rows - 1), (0, EXTRA - seqs * PARTS)))
    carried = carried.reshape(cols, EXTRA)

    last = float(span * devices) * inverse
    last_cosine = jnp.tile(jnp.cos(last), 2 * heads)[None]
    last_sine = jnp.sin(last)
    last_sine = jnp.tile(jnp.concatenate([-last_sine, last_sine]), heads)[None]
    ready = (cosine, sine, weight, carried, last_cosine, last_sine)
    cosine, sine, weight, carried, last_cosine, last_sine = lax.optimization_barrier(ready)

    depth = key_weight.shape[0]
    own, spread = pl.pallas_call(
        spread_kernel,
        out_shape=[
            jax.ShapeDtypeStruct((depth, 2 * cols), BF16),
            jax.ShapeDtypeStruct((Y, depth, 2 * cols), BF16),
        ],
        in_specs=[pl.BlockSpec(memory_space=pl.ANY)] * 2,
        out_specs=[
            pl.BlockSpec(memory_space=pltpu.VMEM),
            pl.BlockSpec(memory_space=pl.ANY),
        ],
        scratch_shapes=[pltpu.SemaphoreType.DMA((2,)), pltpu.SemaphoreType.DMA((2 * Y,))],
    )(key_weight, value_weight)
    sums = projected(tokens.reshape(seqs * span, width), own, spread)
    place = pl.BlockSpec(memory_space=pltpu.SMEM)
    space = pl.BlockSpec(memory_space=pltpu.VMEM)
    lines, value_rows = pl.pallas_call(
        lines_kernel,
        out_shape=[jax.ShapeDtypeStruct((3, lanes), F32), jax.ShapeDtypeStruct((rows, lanes), F32)],
        in_specs=[place] + [space] * 6,
        out_specs=[space] * 2,
        compiler_params=pltpu.CompilerParams(vmem_limit_bytes=2 * 2**20),
    )(
        mine[None],
        last_cosine,
        last_sine,
        new_query,
        new_key,
        new_value,
        step_decay,
    )
    whole = jax.ShapeDtypeStruct((cols, lanes + EXTRA), BF16)

    def exchanged(x):
        cut = x.reshape(devices, rows, lanes + EXTRA)
        return lax.all_to_all(cut, "sp", 0, 0, tiled=True).reshape(x.shape)

    sent = in_vmem(
        functools.partial(share_kernel, seqs), whole, sums, cosine, sine, weight, carried
    )
    finished = in_vmem(
        functools.partial(owner_kernel, devices, seqs), whole, exchanged(sent), lines, value_rows
    )
    state, first_read = in_vmem(
        functools.partial(read_kernel, seqs),
        [jax.ShapeDtypeStruct((cols, lanes), F32), jax.ShapeDtypeStruct((seqs, cols), BF16)],
        exchanged(finished),
        norm_gain.reshape(1, cols),
    )
    state_cache = jnp.transpose(state.reshape(heads, HEAD_DIM, lanes), (2, 0, 1))
    return (state_cache, first_read)


def solution(mesh):
    placed = (
        P("gr", "sp", None),
        P("sp", "tp"),
        P("sp", "tp"),
        P("tp", "gr", "sp"),
        P("gr", "tp"),
        P("gr", "tp"),
        P("gr", "tp"),
        P("tp", "gr"),
        P("tp"),
    )
    return jax.shard_map(
        shards,
        mesh=mesh,
        in_specs=placed,
        out_specs=(P("gr", "tp", None), P("gr", "tp")),
        check_vma=False,
    )
```

```python
import functools

import jax
import jax.numpy as jnp
from jax import lax
from jax.experimental import pallas as pl
from jax.experimental.pallas import tpu as pltpu
from jax.sharding import PartitionSpec as P

HEAD_DIM = 64
Y = 4
PARTS = 3
EXTRA = 128
EXACT = lax.Precision.HIGHEST
F32, BF16 = (jnp.float32, jnp.bfloat16)


def moved_along_z(x, by):
    ring = lax.axis_size("gr") * lax.axis_size("sp") // Y
    pairs = [(z * Y + y, (z + by) % ring * Y + y) for z in range(ring) for y in range(Y)]
    return lax.ppermute(x, ("gr", "sp"), pairs)


def from_opposite_plane(x):
    ring = lax.axis_size("gr") * lax.axis_size("sp") // Y
    wide = lax.axis_size("tp")
    far = lax.axis_size("sp") // Y // 2
    pairs = []
    for z in range(ring):
        for y in range(Y):
            for t in range(wide):
                to = (z + (far if t % 2 else -far)) % ring
                pairs.append(((z * Y + y) * wide + t, (to * Y + y) * wide + t))
    return lax.ppermute(x, ("gr", "sp", "tp"), pairs)


def moved_along_y(x, by):
    planes = lax.axis_size("sp") // Y
    pairs = [(z * Y + y, z * Y + (y + by) % Y) for z in range(planes) for y in range(Y)]
    return lax.ppermute(x, "sp", pairs)


def exchanged_along_y(spread):
    groups = [[z * Y + y for y in range(Y)] for z in range(lax.axis_size("sp") // Y)]
    got = lax.all_to_all(spread, "sp", 0, 0, tiled=True, axis_index_groups=groups)
    return got.reshape(Y * got.shape[1], got.shape[2])


def projected(token_rows, own, spread):
    planes = lax.axis_size("sp") // Y
    far = planes // 2
    mine = lax.axis_index("sp").astype(jnp.uint32) // Y
    block = exchanged_along_y(spread)
    opposite = from_opposite_plane(own)
    depth = block.shape[0]
    row = lax.axis_index("sp").astype(jnp.uint32) % Y

    def part(weights, off, start=0):
        first = (mine + (off + planes)) % planes * depth + start
        cols = lax.dynamic_slice_in_dim(token_rows, first, weights.shape[0], 1)
        return jnp.dot(cols, weights, preferred_element_type=F32)

    def far_part(weights, by):
        return part(weights, far, (row + (Y - by)) % Y * own.shape[0])

    total = part(block, 0)
    up = down = block
    for hop in range(1, far):
        down = moved_along_z(down, -1)
        up = moved_along_z(up, 1)
        beside = moved_along_y(opposite, hop)
        if hop == 1:
            total += far_part(opposite, 0)
        total += far_part(beside, hop) + part(up, -hop) + part(down, hop)
    return total


def in_three(x):
    parts, rest = ([], x)
    for _ in range(PARTS):
        piece = lax.reduce_precision(rest, 8, 7)
        parts.append(piece.astype(jnp.bfloat16))
        rest = rest - piece
    return parts


def lanes_of(shape):
    return lax.broadcasted_iota(jnp.int32, shape, 1)


def rows_of(shape):
    return lax.broadcasted_iota(jnp.int32, shape, 0)


def spread_kernel(key_ref, value_ref, own_ref, spread_ref, sems):
    cols = key_ref.shape[1]
    copies = []
    for ref, cut in ((key_ref, pl.ds(0, cols)), (value_ref, pl.ds(cols, cols))):
        for to in (own_ref.at[:, cut], *(spread_ref.at[y, :, cut] for y in range(Y))):
            copies.append(pltpu.make_async_copy(ref, to, sems.at[len(copies)]))
    for copy in copies:
        copy.start()
    for copy in copies:
        copy.wait()


def share_kernel(seqs, sums_ref, cosine_ref, sine_ref, carried_ref, out_ref):
    cols = out_ref.shape[0]
    heads = cols // HEAD_DIM
    span = sums_ref.shape[0] // seqs
    half = HEAD_DIM // 2
    low = lanes_of((span, cols)) % HEAD_DIM < half
    blocks = [[] for _ in range(heads)]
    for seq in range(seqs):
        here = pl.ds(seq * span, span)
        keys = sums_ref[here, :cols].astype(BF16).astype(F32)
        values = sums_ref[here, cols:].astype(BF16)
        other = jnp.where(low, pltpu.roll(keys, cols - half, 1), pltpu.roll(keys, half, 1))
        faded = keys * cosine_ref[here, :] + other * sine_ref[here, :]
        high = faded.astype(BF16)
        rest = (faded - high.astype(F32)).astype(BF16)
        product = sum(
            lax.dot_general(
                values, part, (((0,), (0,)), ((), ())), preferred_element_type=F32
            )
            for part in (high, rest)
        )
        for head in range(heads):
            cut = slice(head * HEAD_DIM, (head + 1) * HEAD_DIM)
            blocks[head].append(product[cut, cut])
    for head in range(heads):
        cut = pl.ds(head * HEAD_DIM, HEAD_DIM)
        out_ref[cut, : seqs * HEAD_DIM] = jnp.concatenate(blocks[head], axis=1).astype(BF16)
    out_ref[:, seqs * HEAD_DIM :] = carried_ref[...]


def lines_kernel(
    place_ref,
    cosine_ref,
    sine_ref,
    query_ref,
    key_ref,
    value_ref,
    decay_ref,
    table_cosine_ref,
    table_sine_ref,
    weight_ref,
    lines_ref,
    values_ref,
    faded_cosine_ref,
    faded_sine_ref,
):
    seqs, cols = query_ref.shape
    span = table_cosine_ref.shape[0]
    spread = (rows_of((cols // HEAD_DIM, cols)) == lanes_of((cols // HEAD_DIM, cols)) // HEAD_DIM)
    for seq in range(seqs):
        there = pl.ds(seq * span, span)
        weight = jnp.dot(weight_ref[there, :], spread.astype(F32), precision=EXACT)
        faded_cosine_ref[there, :] = table_cosine_ref[...] * weight
        faded_sine_ref[there, :] = table_sine_ref[...] * weight
    heads, lanes = (cols // HEAD_DIM, seqs * HEAD_DIM)
    rows, half = (values_ref.shape[0], HEAD_DIM // 2)
    mine = place_ref[0]
    head = mine * rows // HEAD_DIM
    low = lanes_of((seqs, cols)) % HEAD_DIM < half
    place = (cols, lanes)
    pick = (rows_of(place) // HEAD_DIM == head) & (
        rows_of(place) % HEAD_DIM == lanes_of(place) % HEAD_DIM
    )
    own = rows_of((seqs, lanes)) == lanes_of((seqs, lanes)) // HEAD_DIM

    def line(ref):
        u = ref[...].astype(F32)
        other = jnp.where(low, pltpu.roll(u, cols - half, 1), pltpu.roll(u, half, 1))
        turned = u * cosine_ref[...] + other * sine_ref[...]
        picked = jnp.dot(turned, pick.astype(F32), precision=EXACT)
        return jnp.sum(jnp.where(own, picked, 0.0), axis=0, keepdims=True)

    decay = jnp.dot(jnp.exp(decay_ref[...]), own.astype(F32), precision=EXACT)
    here = rows_of((heads, lanes)) == head
    lines_ref[0:1] = jnp.sum(jnp.where(here, decay, 0.0), axis=0, keepdims=True)
    lines_ref[1:2] = line(key_ref) * HEAD_DIM ** (-0.5)
    lines_ref[2:3] = line(query_ref)
    spot = lanes_of((rows, cols)) == mine * rows + rows_of((rows, cols))
    values = lax.dot_general(
        spot.astype(BF16), value_ref[...], (((1,), (1,)), ((), ())), preferred_element_type=F32
    )
    values_ref[...] = jnp.dot(values, own.astype(F32), precision=EXACT)


def owner_kernel(devices, seqs, got_ref, lines_ref, values_ref, out_ref):
    total, lanes = (got_ref.shape[0], seqs * HEAD_DIM)
    rows = total // devices
    later = (lanes_of((devices, total)) // rows > rows_of((devices, total))) & (
        lanes_of((devices, total)) % rows == 0
    )
    sums = jnp.dot(later.astype(BF16), got_ref[:, lanes:], preferred_element_type=F32)
    place = (EXTRA, lanes)
    wide = (rows_of(place) // PARTS == lanes_of(place) // HEAD_DIM).astype(F32)
    fade = jnp.exp(jnp.dot(sums, wide, precision=EXACT))
    shares = got_ref[:, :lanes].astype(F32)
    owned = shares[:rows] * fade[0:1]
    for device in range(1, devices):
        owned += shares[device * rows : (device + 1) * rows] * fade[device : device + 1]
    finished = lines_ref[0:1] * owned + lines_ref[1:2] * values_ref[...]
    place = (lanes, EXTRA)
    fold = rows_of(place) // HEAD_DIM == lanes_of(place) % seqs
    read = jnp.dot(finished * lines_ref[2:3], fold.astype(F32), precision=EXACT)
    piece = lanes_of(read.shape) // seqs
    rest, packed = (read, jnp.zeros_like(read))
    for part in range(PARTS):
        rounded = rest.astype(BF16).astype(F32)
        packed = jnp.where(piece == part, rounded, packed)
        rest = rest - rounded
    line = jnp.concatenate([finished, packed], axis=1)
    out_ref[...] = jnp.concatenate([line] * devices, axis=0).astype(BF16)


def read_kernel(seqs, got_ref, gain_ref, state_ref, read_ref):
    cols, lanes = (got_ref.shape[0], seqs * HEAD_DIM)
    state_ref[...] = got_ref[:, :lanes].astype(F32)
    place = (8, EXTRA)
    pick = (lanes_of(place) % seqs == rows_of(place)) & (lanes_of(place) < seqs * PARTS)
    raw = lax.dot_general(
        pick.astype(BF16), got_ref[:, lanes:], (((1,), (1,)), ((), ())), preferred_element_type=F32
    )
    place = (cols, cols)
    mean = (rows_of(place) // HEAD_DIM == lanes_of(place) // HEAD_DIM).astype(F32) / HEAD_DIM
    center = raw - jnp.dot(raw, mean, precision=EXACT)
    spread = jnp.dot(center * center, mean, precision=EXACT)
    normed = center * lax.rsqrt(spread + 1e-06) * gain_ref[...]
    read_ref[...] = normed[:seqs].astype(BF16)


def in_vmem(kernel, shapes, *operands):
    space = pl.BlockSpec(memory_space=pltpu.VMEM)
    many = isinstance(shapes, list)
    return pl.pallas_call(
        kernel,
        out_shape=shapes,
        in_specs=[space] * len(operands),
        out_specs=[space] * len(shapes) if many else space,
        compiler_params=pltpu.CompilerParams(vmem_limit_bytes=16 * 2**20),
    )(*operands)


def shards(
    tokens,
    key_weight,
    value_weight,
    log_decay,
    new_query,
    new_key,
    new_value,
    step_decay,
    norm_gain,
):
    seqs, span, width = tokens.shape
    heads = key_weight.shape[1] // HEAD_DIM
    cols = heads * HEAD_DIM
    lanes = seqs * HEAD_DIM
    half = HEAD_DIM // 2
    devices, mine = (lax.axis_size("sp"), lax.axis_index("sp"))
    rows = cols // devices

    positions = (mine * span + jnp.arange(span, dtype=jnp.int32)).astype(F32)
    inverse = 10000.0 ** (-jnp.arange(half, dtype=F32) * (2.0 / HEAD_DIM))
    angles = positions[:, None] * inverse
    cosine = jnp.tile(jnp.cos(angles), (1, 2 * heads)) * HEAD_DIM ** (-0.5)
    sine = jnp.sin(angles) * HEAD_DIM ** (-0.5)
    sine = jnp.tile(jnp.concatenate([-sine, sine], axis=1), (1, heads))
    totals = jnp.sum(log_decay, axis=-1)
    weight = jnp.exp(totals[:, :, None] - jnp.cumsum(log_decay, axis=-1))
    weight = jnp.transpose(weight, (1, 2, 0)).reshape(seqs * span, heads)
    carried = jnp.stack(in_three(totals), axis=-1).reshape(heads, 1, 1, seqs * PARTS)
    carried = jnp.broadcast_to(carried, (heads, devices // heads, 1, seqs * PARTS))
    carried = carried.reshape(devices, 1, seqs * PARTS)
    carried = jnp.pad(carried, ((0, 0), (0, rows - 1), (0, EXTRA - seqs * PARTS)))
    carried = carried.reshape(cols, EXTRA)

    last = float(span * devices) * inverse
    last_cosine = jnp.tile(jnp.cos(last), 2 * heads)[None]
    last_sine = jnp.sin(last)
    last_sine = jnp.tile(jnp.concatenate([-last_sine, last_sine]), heads)[None]
    ready = (cosine, sine, weight, carried, last_cosine, last_sine)
    cosine, sine, weight, carried, last_cosine, last_sine = lax.optimization_barrier(ready)

    depth = key_weight.shape[0]
    own, spread = pl.pallas_call(
        spread_kernel,
        out_shape=[
            jax.ShapeDtypeStruct((depth, 2 * cols), BF16),
            jax.ShapeDtypeStruct((Y, depth, 2 * cols), BF16),
        ],
        in_specs=[pl.BlockSpec(memory_space=pl.ANY)] * 2,
        out_specs=[pl.BlockSpec(memory_space=pltpu.VMEM)] * 2,
        scratch_shapes=[pltpu.SemaphoreType.DMA((2 * (Y + 1),))],
    )(key_weight, value_weight)
    sums = projected(tokens.reshape(seqs * span, width), own, spread)
    place = pl.BlockSpec(memory_space=pltpu.SMEM)
    space = pl.BlockSpec(memory_space=pltpu.VMEM)
    lines, value_rows, cosine, sine = pl.pallas_call(
        lines_kernel,
        out_shape=[
            jax.ShapeDtypeStruct((3, lanes), F32),
            jax.ShapeDtypeStruct((rows, lanes), F32),
            jax.ShapeDtypeStruct((seqs * span, cols), F32),
            jax.ShapeDtypeStruct((seqs * span, cols), F32),
        ],
        in_specs=[place] + [space] * 9,
        out_specs=[space] * 4,
        compiler_params=pltpu.CompilerParams(vmem_limit_bytes=6 * 2**20),
    )(
        mine[None],
        last_cosine,
        last_sine,
        new_query,
        new_key,
        new_value,
        step_decay,
        cosine,
        sine,
        weight,
    )
    whole = jax.ShapeDtypeStruct((cols, lanes + EXTRA), BF16)

    def exchanged(x):
        cut = x.reshape(devices, rows, lanes + EXTRA)
        return lax.all_to_all(cut, "sp", 0, 0, tiled=True).reshape(x.shape)

    sent = in_vmem(
        functools.partial(share_kernel, seqs), whole, sums, cosine, sine, carried
    )
    finished = in_vmem(
        functools.partial(owner_kernel, devices, seqs), whole, exchanged(sent), lines, value_rows
    )
    state, first_read = in_vmem(
        functools.partial(read_kernel, seqs),
        [jax.ShapeDtypeStruct((cols, lanes), F32), jax.ShapeDtypeStruct((seqs, cols), BF16)],
        exchanged(finished),
        norm_gain.reshape(1, cols),
    )
    state_cache = jnp.transpose(state.reshape(heads, HEAD_DIM, lanes), (2, 0, 1))
    return (state_cache, first_read)


def solution(mesh):
    placed = (
        P("gr", "sp", None),
        P("sp", "tp"),
        P("sp", "tp"),
        P("tp", "gr", "sp"),
        P("gr", "tp"),
        P("gr", "tp"),
        P("gr", "tp"),
        P("tp", "gr"),
        P("tp"),
    )
    return jax.shard_map(
        shards,
        mesh=mesh,
        in_specs=placed,
        out_specs=(P("gr", "tp", None), P("gr", "tp")),
        check_vma=False,
    )
```

```python
import functools

import jax
import jax.numpy as jnp
from jax import lax
from jax.experimental import pallas as pl
from jax.experimental.pallas import tpu as pltpu
from jax.sharding import PartitionSpec as P

HEAD_DIM = 64
Y = 4
PARTS = 3
EXTRA = 128
F32, BF16 = (jnp.float32, jnp.bfloat16)


def moved_along_z(x, by):
    ring = lax.axis_size("gr") * lax.axis_size("sp") // Y
    pairs = [(z * Y + y, (z + by) % ring * Y + y) for z in range(ring) for y in range(Y)]
    return lax.ppermute(x, ("gr", "sp"), pairs)


def from_opposite_plane(x):
    ring = lax.axis_size("gr") * lax.axis_size("sp") // Y
    wide = lax.axis_size("tp")
    far = lax.axis_size("sp") // Y // 2
    pairs = []
    for z in range(ring):
        for y in range(Y):
            for t in range(wide):
                to = (z + (far if t % 2 else -far)) % ring
                pairs.append(((z * Y + y) * wide + t, (to * Y + y) * wide + t))
    return lax.ppermute(x, ("gr", "sp", "tp"), pairs)


def moved_along_y(x, by):
    planes = lax.axis_size("sp") // Y
    pairs = [(z * Y + y, z * Y + (y + by) % Y) for z in range(planes) for y in range(Y)]
    return lax.ppermute(x, "sp", pairs)


def exchanged_along_y(spread):
    groups = [[z * Y + y for y in range(Y)] for z in range(lax.axis_size("sp") // Y)]
    got = lax.all_to_all(spread, "sp", 0, 0, tiled=True, axis_index_groups=groups)
    return got.reshape(Y * got.shape[1], got.shape[2])


def projected(token_rows, own, spread):
    planes = lax.axis_size("sp") // Y
    far = planes // 2
    mine = lax.axis_index("sp").astype(jnp.uint32) // Y
    block = exchanged_along_y(spread)
    opposite = from_opposite_plane(own)
    depth = block.shape[0]
    row = lax.axis_index("sp").astype(jnp.uint32) % Y

    def part(weights, off, start=0):
        first = (mine + (off + planes)) % planes * depth + start
        cols = lax.dynamic_slice_in_dim(token_rows, first, weights.shape[0], 1)
        return jnp.dot(cols, weights, preferred_element_type=F32)

    def far_part(weights, by):
        return part(weights, far, (row + (Y - by)) % Y * own.shape[0])

    total = part(block, 0)
    up = down = block
    for hop in range(1, far):
        down = moved_along_z(down, -1)
        up = moved_along_z(up, 1)
        beside = moved_along_y(opposite, hop)
        if hop == 1:
            total += far_part(opposite, 0)
        total += far_part(beside, hop) + part(up, -hop) + part(down, hop)
    return total


def in_three(x):
    parts, rest = ([], x)
    for _ in range(PARTS):
        piece = lax.reduce_precision(rest, 8, 7)
        parts.append(piece.astype(jnp.bfloat16))
        rest = rest - piece
    return parts


def lanes_of(shape):
    return lax.broadcasted_iota(jnp.int32, shape, 1)


def rows_of(shape):
    return lax.broadcasted_iota(jnp.int32, shape, 0)


def spread_kernel(key_ref, value_ref, own_ref, spread_ref, sems):
    cols = key_ref.shape[1]
    copies = []
    for ref, cut in ((key_ref, pl.ds(0, cols)), (value_ref, pl.ds(cols, cols))):
        for to in (own_ref.at[:, cut], *(spread_ref.at[y, :, cut] for y in range(Y))):
            copies.append(pltpu.make_async_copy(ref, to, sems.at[len(copies)]))
    for copy in copies:
        copy.start()
    for copy in copies:
        copy.wait()


def summed_where(x, chosen):
    chosen, total = (chosen.astype(BF16), None)
    for _ in range(PARTS):
        part = x.astype(BF16)
        product = jnp.dot(part, chosen, preferred_element_type=F32)
        total = product if total is None else total + product
        x = x - part.astype(F32)
    return total


def share_kernel(seqs, sums_ref, cosine_ref, sine_ref, carried_ref, out_ref):
    cols = out_ref.shape[0]
    heads = cols // HEAD_DIM
    span = sums_ref.shape[0] // seqs
    half = HEAD_DIM // 2
    low = lanes_of((span, cols)) % HEAD_DIM < half
    blocks = [[] for _ in range(heads)]
    for seq in range(seqs):
        here = pl.ds(seq * span, span)
        keys = sums_ref[here, :cols].astype(BF16).astype(F32)
        values = sums_ref[here, cols:].astype(BF16)
        other = jnp.where(low, pltpu.roll(keys, cols - half, 1), pltpu.roll(keys, half, 1))
        faded = keys * cosine_ref[here, :] + other * sine_ref[here, :]
        high = faded.astype(BF16)
        rest = (faded - high.astype(F32)).astype(BF16)
        product = sum(
            lax.dot_general(
                values, part, (((0,), (0,)), ((), ())), preferred_element_type=F32
            )
            for part in (high, rest)
        )
        for head in range(heads):
            cut = slice(head * HEAD_DIM, (head + 1) * HEAD_DIM)
            blocks[head].append(product[cut, cut])
    for head in range(heads):
        cut = pl.ds(head * HEAD_DIM, HEAD_DIM)
        out_ref[cut, : seqs * HEAD_DIM] = jnp.concatenate(blocks[head], axis=1).astype(BF16)
    out_ref[:, seqs * HEAD_DIM :] = carried_ref[...]


def lines_kernel(
    place_ref,
    cosine_ref,
    sine_ref,
    query_ref,
    key_ref,
    value_ref,
    decay_ref,
    table_cosine_ref,
    table_sine_ref,
    weight_ref,
    lines_ref,
    values_ref,
    faded_cosine_ref,
    faded_sine_ref,
):
    seqs, cols = query_ref.shape
    span = table_cosine_ref.shape[0]
    spread = (rows_of((cols // HEAD_DIM, cols)) == lanes_of((cols // HEAD_DIM, cols)) // HEAD_DIM)
    for seq in range(seqs):
        there = pl.ds(seq * span, span)
        weight = summed_where(weight_ref[there, :], spread)
        faded_cosine_ref[there, :] = table_cosine_ref[...] * weight
        faded_sine_ref[there, :] = table_sine_ref[...] * weight
    heads, lanes = (cols // HEAD_DIM, seqs * HEAD_DIM)
    rows, half = (values_ref.shape[0], HEAD_DIM // 2)
    mine = place_ref[0]
    head = mine * rows // HEAD_DIM
    low = lanes_of((seqs, cols)) % HEAD_DIM < half
    place = (cols, lanes)
    pick = (rows_of(place) // HEAD_DIM == head) & (
        rows_of(place) % HEAD_DIM == lanes_of(place) % HEAD_DIM
    )
    own = rows_of((seqs, lanes)) == lanes_of((seqs, lanes)) // HEAD_DIM

    def line(ref):
        u = ref[...].astype(F32)
        other = jnp.where(low, pltpu.roll(u, cols - half, 1), pltpu.roll(u, half, 1))
        turned = u * cosine_ref[...] + other * sine_ref[...]
        picked = summed_where(turned, pick)
        return jnp.sum(jnp.where(own, picked, 0.0), axis=0, keepdims=True)

    decay = summed_where(jnp.exp(decay_ref[...]), own)
    here = rows_of((heads, lanes)) == head
    lines_ref[0:1] = jnp.sum(jnp.where(here, decay, 0.0), axis=0, keepdims=True)
    lines_ref[1:2] = line(key_ref) * HEAD_DIM ** (-0.5)
    lines_ref[2:3] = line(query_ref)
    spot = lanes_of((rows, cols)) == mine * rows + rows_of((rows, cols))
    values = lax.dot_general(
        spot.astype(BF16), value_ref[...], (((1,), (1,)), ((), ())), preferred_element_type=F32
    )
    values_ref[...] = summed_where(values, own)


def owner_kernel(devices, seqs, got_ref, lines_ref, values_ref, out_ref):
    total, lanes = (got_ref.shape[0], seqs * HEAD_DIM)
    rows = total // devices
    later = (lanes_of((devices, total)) // rows > rows_of((devices, total))) & (
        lanes_of((devices, total)) % rows == 0
    )
    sums = jnp.dot(later.astype(BF16), got_ref[:, lanes:], preferred_element_type=F32)
    place = (EXTRA, lanes)
    wide = rows_of(place) // PARTS == lanes_of(place) // HEAD_DIM
    fade = jnp.exp(summed_where(sums, wide))
    shares = got_ref[:, :lanes].astype(F32)
    owned = shares[:rows] * fade[0:1]
    for device in range(1, devices):
        owned += shares[device * rows : (device + 1) * rows] * fade[device : device + 1]
    finished = lines_ref[0:1] * owned + lines_ref[1:2] * values_ref[...]
    place = (lanes, EXTRA)
    fold = rows_of(place) // HEAD_DIM == lanes_of(place) % seqs
    read = summed_where(finished * lines_ref[2:3], fold)
    piece = lanes_of(read.shape) // seqs
    rest, packed = (read, jnp.zeros_like(read))
    for part in range(PARTS):
        rounded = rest.astype(BF16).astype(F32)
        packed = jnp.where(piece == part, rounded, packed)
        rest = rest - rounded
    line = jnp.concatenate([finished, packed], axis=1)
    out_ref[...] = jnp.concatenate([line] * devices, axis=0).astype(BF16)


def read_kernel(seqs, got_ref, gain_ref, state_ref, read_ref):
    cols, lanes = (got_ref.shape[0], seqs * HEAD_DIM)
    state_ref[...] = got_ref[:, :lanes].astype(F32)
    place = (8, EXTRA)
    pick = (lanes_of(place) % seqs == rows_of(place)) & (lanes_of(place) < seqs * PARTS)
    raw = lax.dot_general(
        pick.astype(BF16), got_ref[:, lanes:], (((1,), (1,)), ((), ())), preferred_element_type=F32
    )
    place = (cols, cols)
    head = rows_of(place) // HEAD_DIM == lanes_of(place) // HEAD_DIM
    center = raw - summed_where(raw, head) / HEAD_DIM
    spread = summed_where(center * center, head) / HEAD_DIM
    normed = center * lax.rsqrt(spread + 1e-06) * gain_ref[...]
    read_ref[...] = normed[:seqs].astype(BF16)


def in_vmem(kernel, shapes, *operands):
    space = pl.BlockSpec(memory_space=pltpu.VMEM)
    many = isinstance(shapes, list)
    return pl.pallas_call(
        kernel,
        out_shape=shapes,
        in_specs=[space] * len(operands),
        out_specs=[space] * len(shapes) if many else space,
        compiler_params=pltpu.CompilerParams(vmem_limit_bytes=16 * 2**20),
    )(*operands)


def shards(
    tokens,
    key_weight,
    value_weight,
    log_decay,
    new_query,
    new_key,
    new_value,
    step_decay,
    norm_gain,
):
    seqs, span, width = tokens.shape
    heads = key_weight.shape[1] // HEAD_DIM
    cols = heads * HEAD_DIM
    lanes = seqs * HEAD_DIM
    half = HEAD_DIM // 2
    devices, mine = (lax.axis_size("sp"), lax.axis_index("sp"))
    rows = cols // devices

    positions = (mine * span + jnp.arange(span, dtype=jnp.int32)).astype(F32)
    inverse = 10000.0 ** (-jnp.arange(half, dtype=F32) * (2.0 / HEAD_DIM))
    angles = positions[:, None] * inverse
    cosine = jnp.tile(jnp.cos(angles), (1, 2 * heads)) * HEAD_DIM ** (-0.5)
    sine = jnp.sin(angles) * HEAD_DIM ** (-0.5)
    sine = jnp.tile(jnp.concatenate([-sine, sine], axis=1), (1, heads))
    totals = jnp.sum(log_decay, axis=-1)
    weight = jnp.exp(totals[:, :, None] - jnp.cumsum(log_decay, axis=-1))
    weight = jnp.transpose(weight, (1, 2, 0)).reshape(seqs * span, heads)
    carried = jnp.stack(in_three(totals), axis=-1).reshape(heads, 1, 1, seqs * PARTS)
    carried = jnp.broadcast_to(carried, (heads, devices // heads, 1, seqs * PARTS))
    carried = carried.reshape(devices, 1, seqs * PARTS)
    carried = jnp.pad(carried, ((0, 0), (0, rows - 1), (0, EXTRA - seqs * PARTS)))
    carried = carried.reshape(cols, EXTRA)

    last = float(span * devices) * inverse
    last_cosine = jnp.tile(jnp.cos(last), 2 * heads)[None]
    last_sine = jnp.sin(last)
    last_sine = jnp.tile(jnp.concatenate([-last_sine, last_sine]), heads)[None]
    ready = (cosine, sine, weight, carried, last_cosine, last_sine)
    cosine, sine, weight, carried, last_cosine, last_sine = lax.optimization_barrier(ready)

    depth = key_weight.shape[0]
    own, spread = pl.pallas_call(
        spread_kernel,
        out_shape=[
            jax.ShapeDtypeStruct((depth, 2 * cols), BF16),
            jax.ShapeDtypeStruct((Y, depth, 2 * cols), BF16),
        ],
        in_specs=[pl.BlockSpec(memory_space=pl.ANY)] * 2,
        out_specs=[pl.BlockSpec(memory_space=pltpu.VMEM)] * 2,
        scratch_shapes=[pltpu.SemaphoreType.DMA((2 * (Y + 1),))],
    )(key_weight, value_weight)
    sums = projected(tokens.reshape(seqs * span, width), own, spread)
    place = pl.BlockSpec(memory_space=pltpu.SMEM)
    space = pl.BlockSpec(memory_space=pltpu.VMEM)
    lines, value_rows, cosine, sine = pl.pallas_call(
        lines_kernel,
        out_shape=[
            jax.ShapeDtypeStruct((3, lanes), F32),
            jax.ShapeDtypeStruct((rows, lanes), F32),
            jax.ShapeDtypeStruct((seqs * span, cols), F32),
            jax.ShapeDtypeStruct((seqs * span, cols), F32),
        ],
        in_specs=[place] + [space] * 9,
        out_specs=[space] * 4,
        compiler_params=pltpu.CompilerParams(vmem_limit_bytes=6 * 2**20),
    )(
        mine[None],
        last_cosine,
        last_sine,
        new_query,
        new_key,
        new_value,
        step_decay,
        cosine,
        sine,
        weight,
    )
    whole = jax.ShapeDtypeStruct((cols, lanes + EXTRA), BF16)

    def exchanged(x):
        cut = x.reshape(devices, rows, lanes + EXTRA)
        return lax.all_to_all(cut, "sp", 0, 0, tiled=True).reshape(x.shape)

    sent = in_vmem(
        functools.partial(share_kernel, seqs), whole, sums, cosine, sine, carried
    )
    finished = in_vmem(
        functools.partial(owner_kernel, devices, seqs), whole, exchanged(sent), lines, value_rows
    )
    state, first_read = in_vmem(
        functools.partial(read_kernel, seqs),
        [jax.ShapeDtypeStruct((cols, lanes), F32), jax.ShapeDtypeStruct((seqs, cols), BF16)],
        exchanged(finished),
        norm_gain.reshape(1, cols),
    )
    state_cache = jnp.transpose(state.reshape(heads, HEAD_DIM, lanes), (2, 0, 1))
    return (state_cache, first_read)


def solution(mesh):
    placed = (
        P("gr", "sp", None),
        P("sp", "tp"),
        P("sp", "tp"),
        P("tp", "gr", "sp"),
        P("gr", "tp"),
        P("gr", "tp"),
        P("gr", "tp"),
        P("tp", "gr"),
        P("tp"),
    )
    return jax.shard_map(
        shards,
        mesh=mesh,
        in_specs=placed,
        out_specs=(P("gr", "tp", None), P("gr", "tp")),
        check_vma=False,
    )
```

```python
import functools

import jax
import jax.numpy as jnp
from jax import lax
from jax.experimental import pallas as pl
from jax.experimental.pallas import tpu as pltpu
from jax.sharding import PartitionSpec as P

HEAD_DIM = 64
Y = 4
PARTS = 3
EXTRA = 128
F32, BF16 = (jnp.float32, jnp.bfloat16)


def moved_along_z(x, by):
    ring = lax.axis_size("gr") * lax.axis_size("sp") // Y
    pairs = [(z * Y + y, (z + by) % ring * Y + y) for z in range(ring) for y in range(Y)]
    return lax.ppermute(x, ("gr", "sp"), pairs)


def from_opposite_plane(x):
    ring = lax.axis_size("gr") * lax.axis_size("sp") // Y
    wide = lax.axis_size("tp")
    far = lax.axis_size("sp") // Y // 2
    pairs = []
    for z in range(ring):
        for y in range(Y):
            for t in range(wide):
                to = (z + (far if t % 2 else -far)) % ring
                pairs.append(((z * Y + y) * wide + t, (to * Y + y) * wide + t))
    return lax.ppermute(x, ("gr", "sp", "tp"), pairs)


def moved_along_y(x, by):
    planes = lax.axis_size("sp") // Y
    pairs = [(z * Y + y, z * Y + (y + by) % Y) for z in range(planes) for y in range(Y)]
    return lax.ppermute(x, "sp", pairs)


def exchanged_along_y(spread):
    groups = [[z * Y + y for y in range(Y)] for z in range(lax.axis_size("sp") // Y)]
    got = lax.all_to_all(spread, "sp", 0, 0, tiled=True, axis_index_groups=groups)
    return got.reshape(Y * got.shape[1], got.shape[2])


def projected(token_rows, own, spread):
    planes = lax.axis_size("sp") // Y
    far = planes // 2
    mine = lax.axis_index("sp").astype(jnp.uint32) // Y
    block = exchanged_along_y(spread)
    opposite = from_opposite_plane(own)
    depth = block.shape[0]
    row = lax.axis_index("sp").astype(jnp.uint32) % Y

    def part(weights, off, start=0):
        first = (mine + (off + planes)) % planes * depth + start
        cols = lax.dynamic_slice_in_dim(token_rows, first, weights.shape[0], 1)
        return jnp.dot(cols, weights, preferred_element_type=F32)

    def far_part(weights, by):
        return part(weights, far, (row + (Y - by)) % Y * own.shape[0])

    total = part(block, 0)
    up = down = block
    for hop in range(1, far):
        down = moved_along_z(down, -1)
        up = moved_along_z(up, 1)
        beside = moved_along_y(opposite, hop)
        if hop == 1:
            total += far_part(opposite, 0)
        total += far_part(beside, hop) + part(up, -hop) + part(down, hop)
    return total


def in_three(x):
    parts, rest = ([], x)
    for _ in range(PARTS):
        piece = lax.reduce_precision(rest, 8, 7)
        parts.append(piece.astype(jnp.bfloat16))
        rest = rest - piece
    return parts


def lanes_of(shape):
    return lax.broadcasted_iota(jnp.int32, shape, 1)


def rows_of(shape):
    return lax.broadcasted_iota(jnp.int32, shape, 0)


def spread_kernel(key_ref, value_ref, own_ref, spread_ref, both_ref, in_sems, out_sems):
    cols = key_ref.shape[1]
    loads = [
        pltpu.make_async_copy(ref, both_ref.at[:, pl.ds(n * cols, cols)], in_sems.at[n])
        for n, ref in enumerate((key_ref, value_ref))
    ]
    for load in loads:
        load.start()
    for load in loads:
        load.wait()
    places = (*(spread_ref.at[y] for y in range(Y)), own_ref)
    copies = [
        pltpu.make_async_copy(both_ref, to, out_sems.at[n]) for n, to in enumerate(places)
    ]
    for copy in copies:
        copy.start()
    for copy in copies:
        copy.wait()


def summed_where(x, chosen):
    chosen, total = (chosen.astype(BF16), None)
    for _ in range(PARTS):
        part = x.astype(BF16)
        product = jnp.dot(part, chosen, preferred_element_type=F32)
        total = product if total is None else total + product
        x = x - part.astype(F32)
    return total


def share_kernel(seqs, sums_ref, cosine_ref, sine_ref, carried_ref, out_ref):
    cols = out_ref.shape[0]
    heads = cols // HEAD_DIM
    span = sums_ref.shape[0] // seqs
    half = HEAD_DIM // 2
    low = lanes_of((span, cols)) % HEAD_DIM < half
    blocks = [[] for _ in range(heads)]
    for seq in range(seqs):
        here = pl.ds(seq * span, span)
        keys = sums_ref[here, :cols].astype(BF16).astype(F32)
        values = sums_ref[here, cols:].astype(BF16)
        other = jnp.where(low, pltpu.roll(keys, cols - half, 1), pltpu.roll(keys, half, 1))
        faded = keys * cosine_ref[here, :] + other * sine_ref[here, :]
        high = faded.astype(BF16)
        rest = (faded - high.astype(F32)).astype(BF16)
        product = sum(
            lax.dot_general(
                values, part, (((0,), (0,)), ((), ())), preferred_element_type=F32
            )
            for part in (high, rest)
        )
        for head in range(heads):
            cut = slice(head * HEAD_DIM, (head + 1) * HEAD_DIM)
            blocks[head].append(product[cut, cut])
    for head in range(heads):
        cut = pl.ds(head * HEAD_DIM, HEAD_DIM)
        out_ref[cut, : seqs * HEAD_DIM] = jnp.concatenate(blocks[head], axis=1).astype(BF16)
    out_ref[:, seqs * HEAD_DIM :] = carried_ref[...]


def lines_kernel(
    place_ref,
    cosine_ref,
    sine_ref,
    query_ref,
    key_ref,
    value_ref,
    decay_ref,
    table_cosine_ref,
    table_sine_ref,
    weight_ref,
    lines_ref,
    values_ref,
    faded_cosine_ref,
    faded_sine_ref,
):
    seqs, cols = query_ref.shape
    span = table_cosine_ref.shape[0]
    spread = (rows_of((cols // HEAD_DIM, cols)) == lanes_of((cols // HEAD_DIM, cols)) // HEAD_DIM)
    for seq in range(seqs):
        there = pl.ds(seq * span, span)
        weight = summed_where(weight_ref[there, :], spread)
        faded_cosine_ref[there, :] = table_cosine_ref[...] * weight
        faded_sine_ref[there, :] = table_sine_ref[...] * weight
    heads, lanes = (cols // HEAD_DIM, seqs * HEAD_DIM)
    rows, half = (values_ref.shape[0], HEAD_DIM // 2)
    mine = place_ref[0]
    head = mine * rows // HEAD_DIM
    low = lanes_of((seqs, cols)) % HEAD_DIM < half
    place = (cols, lanes)
    pick = (rows_of(place) // HEAD_DIM == head) & (
        rows_of(place) % HEAD_DIM == lanes_of(place) % HEAD_DIM
    )
    own = rows_of((seqs, lanes)) == lanes_of((seqs, lanes)) // HEAD_DIM

    def line(ref):
        u = ref[...].astype(F32)
        other = jnp.where(low, pltpu.roll(u, cols - half, 1), pltpu.roll(u, half, 1))
        turned = u * cosine_ref[...] + other * sine_ref[...]
        picked = summed_where(turned, pick)
        return jnp.sum(jnp.where(own, picked, 0.0), axis=0, keepdims=True)

    decay = summed_where(jnp.exp(decay_ref[...]), own)
    here = rows_of((heads, lanes)) == head
    lines_ref[0:1] = jnp.sum(jnp.where(here, decay, 0.0), axis=0, keepdims=True)
    lines_ref[1:2] = line(key_ref) * HEAD_DIM ** (-0.5)
    lines_ref[2:3] = line(query_ref)
    spot = lanes_of((rows, cols)) == mine * rows + rows_of((rows, cols))
    values = lax.dot_general(
        spot.astype(BF16), value_ref[...], (((1,), (1,)), ((), ())), preferred_element_type=F32
    )
    values_ref[...] = summed_where(values, own)


def owner_kernel(devices, seqs, got_ref, lines_ref, values_ref, out_ref):
    total, lanes = (got_ref.shape[0], seqs * HEAD_DIM)
    rows = total // devices
    later = (lanes_of((devices, total)) // rows > rows_of((devices, total))) & (
        lanes_of((devices, total)) % rows == 0
    )
    sums = jnp.dot(later.astype(BF16), got_ref[:, lanes:], preferred_element_type=F32)
    place = (EXTRA, lanes)
    wide = rows_of(place) // PARTS == lanes_of(place) // HEAD_DIM
    fade = jnp.exp(summed_where(sums, wide))
    shares = got_ref[:, :lanes].astype(F32)
    owned = shares[:rows] * fade[0:1]
    for device in range(1, devices):
        owned += shares[device * rows : (device + 1) * rows] * fade[device : device + 1]
    finished = lines_ref[0:1] * owned + lines_ref[1:2] * values_ref[...]
    place = (lanes, EXTRA)
    fold = rows_of(place) // HEAD_DIM == lanes_of(place) % seqs
    read = summed_where(finished * lines_ref[2:3], fold)
    piece = lanes_of(read.shape) // seqs
    rest, packed = (read, jnp.zeros_like(read))
    for part in range(PARTS):
        rounded = rest.astype(BF16).astype(F32)
        packed = jnp.where(piece == part, rounded, packed)
        rest = rest - rounded
    line = jnp.concatenate([finished, packed], axis=1)
    out_ref[...] = jnp.concatenate([line] * devices, axis=0).astype(BF16)


def read_kernel(seqs, got_ref, gain_ref, state_ref, read_ref):
    cols, lanes = (got_ref.shape[0], seqs * HEAD_DIM)
    state_ref[...] = got_ref[:, :lanes].astype(F32)
    place = (8, EXTRA)
    pick = (lanes_of(place) % seqs == rows_of(place)) & (lanes_of(place) < seqs * PARTS)
    raw = lax.dot_general(
        pick.astype(BF16), got_ref[:, lanes:], (((1,), (1,)), ((), ())), preferred_element_type=F32
    )
    place = (cols, cols)
    head = rows_of(place) // HEAD_DIM == lanes_of(place) // HEAD_DIM
    center = raw - summed_where(raw, head) / HEAD_DIM
    spread = summed_where(center * center, head) / HEAD_DIM
    normed = center * lax.rsqrt(spread + 1e-06) * gain_ref[...]
    read_ref[...] = normed[:seqs].astype(BF16)


def in_vmem(kernel, shapes, *operands):
    space = pl.BlockSpec(memory_space=pltpu.VMEM)
    many = isinstance(shapes, list)
    return pl.pallas_call(
        kernel,
        out_shape=shapes,
        in_specs=[space] * len(operands),
        out_specs=[space] * len(shapes) if many else space,
        compiler_params=pltpu.CompilerParams(vmem_limit_bytes=16 * 2**20),
    )(*operands)


def shards(
    tokens,
    key_weight,
    value_weight,
    log_decay,
    new_query,
    new_key,
    new_value,
    step_decay,
    norm_gain,
):
    seqs, span, width = tokens.shape
    heads = key_weight.shape[1] // HEAD_DIM
    cols = heads * HEAD_DIM
    lanes = seqs * HEAD_DIM
    half = HEAD_DIM // 2
    devices, mine = (lax.axis_size("sp"), lax.axis_index("sp"))
    rows = cols // devices

    positions = (mine * span + jnp.arange(span, dtype=jnp.int32)).astype(F32)
    inverse = 10000.0 ** (-jnp.arange(half, dtype=F32) * (2.0 / HEAD_DIM))
    angles = positions[:, None] * inverse
    cosine = jnp.tile(jnp.cos(angles), (1, 2 * heads)) * HEAD_DIM ** (-0.5)
    sine = jnp.sin(angles) * HEAD_DIM ** (-0.5)
    sine = jnp.tile(jnp.concatenate([-sine, sine], axis=1), (1, heads))
    totals = jnp.sum(log_decay, axis=-1)
    summed = jnp.cumsum(log_decay, axis=-1)
    weight = jnp.exp(totals[:, :, None] - summed)
    weight = jnp.transpose(weight, (1, 2, 0)).reshape(seqs * span, heads)
    carried = jnp.stack(in_three(totals), axis=-1).reshape(heads, 1, 1, seqs * PARTS)
    carried = jnp.broadcast_to(carried, (heads, devices // heads, 1, seqs * PARTS))
    carried = carried.reshape(devices, 1, seqs * PARTS)
    carried = jnp.pad(carried, ((0, 0), (0, rows - 1), (0, EXTRA - seqs * PARTS)))
    carried = carried.reshape(cols, EXTRA)

    last = float(span * devices) * inverse
    last_cosine = jnp.tile(jnp.cos(last), 2 * heads)[None]
    last_sine = jnp.sin(last)
    last_sine = jnp.tile(jnp.concatenate([-last_sine, last_sine]), heads)[None]
    ready = (cosine, sine, weight, carried, last_cosine, last_sine)
    cosine, sine, weight, carried, last_cosine, last_sine = lax.optimization_barrier(ready)

    depth = key_weight.shape[0]
    own, spread = pl.pallas_call(
        spread_kernel,
        out_shape=[
            jax.ShapeDtypeStruct((depth, 2 * cols), BF16),
            jax.ShapeDtypeStruct((Y, depth, 2 * cols), BF16),
        ],
        in_specs=[pl.BlockSpec(memory_space=pl.ANY)] * 2,
        out_specs=[pl.BlockSpec(memory_space=pl.ANY)] * 2,
        scratch_shapes=[
            pltpu.VMEM((depth, 2 * cols), BF16),
            pltpu.SemaphoreType.DMA((2,)),
            pltpu.SemaphoreType.DMA((Y + 1,)),
        ],
    )(key_weight, value_weight)
    sums = projected(tokens.reshape(seqs * span, width), own, spread)
    place = pl.BlockSpec(memory_space=pltpu.SMEM)
    space = pl.BlockSpec(memory_space=pltpu.VMEM)
    lines, value_rows, cosine, sine = pl.pallas_call(
        lines_kernel,
        out_shape=[
            jax.ShapeDtypeStruct((3, lanes), F32),
            jax.ShapeDtypeStruct((rows, lanes), F32),
            jax.ShapeDtypeStruct((seqs * span, cols), F32),
            jax.ShapeDtypeStruct((seqs * span, cols), F32),
        ],
        in_specs=[place] + [space] * 9,
        out_specs=[space] * 4,
        compiler_params=pltpu.CompilerParams(vmem_limit_bytes=6 * 2**20),
    )(
        mine[None],
        last_cosine,
        last_sine,
        new_query,
        new_key,
        new_value,
        step_decay,
        cosine,
        sine,
        weight,
    )
    whole = jax.ShapeDtypeStruct((cols, lanes + EXTRA), BF16)

    def exchanged(x):
        cut = x.reshape(devices, rows, lanes + EXTRA)
        return lax.all_to_all(cut, "sp", 0, 0, tiled=True).reshape(x.shape)

    sent = in_vmem(
        functools.partial(share_kernel, seqs), whole, sums, cosine, sine, carried
    )
    finished = in_vmem(
        functools.partial(owner_kernel, devices, seqs), whole, exchanged(sent), lines, value_rows
    )
    state, first_read = in_vmem(
        functools.partial(read_kernel, seqs),
        [jax.ShapeDtypeStruct((cols, lanes), F32), jax.ShapeDtypeStruct((seqs, cols), BF16)],
        exchanged(finished),
        norm_gain.reshape(1, cols),
    )
    state_cache = jnp.transpose(state.reshape(heads, HEAD_DIM, lanes), (2, 0, 1))
    return (state_cache, first_read)


def solution(mesh):
    placed = (
        P("gr", "sp", None),
        P("sp", "tp"),
        P("sp", "tp"),
        P("tp", "gr", "sp"),
        P("gr", "tp"),
        P("gr", "tp"),
        P("gr", "tp"),
        P("tp", "gr"),
        P("tp"),
    )
    return jax.shard_map(
        shards,
        mesh=mesh,
        in_specs=placed,
        out_specs=(P("gr", "tp", None), P("gr", "tp")),
        check_vma=False,
    )
```
